32 devices in a mesh: sp: 4 (over z), fs: 4 (over y, x), tp: 2 (over core).
Axes of the slice: x: 2, y: 2, z: 4, core: 2. Of those that a mesh axis runs over, the one named last changes fastest.
Arguments:
- tokens: bfloat16 [6144, 2048], P(('fs', 'sp', 'tp')), parts along dimension 0, may hold values from -6 to 6
- norm_gain: float32 [2048], replicated, may hold values from 0.1 to 1.9
- w_input: bfloat16 [2048, 1024], P(None, 'tp'), may hold values from -0.125 to 0.125
- w_query: bfloat16 [2048, 1024], P(None, 'tp'), may hold values from -0.125 to 0.125
- w_key: bfloat16 [2048, 1024], P(None, 'tp'), may hold values from -0.125 to 0.125
- w_value: bfloat16 [2048, 1024], P(None, 'tp'), may hold values from -0.125 to 0.125
- query_gain: float32 [64], replicated, may hold values from 0.1 to 1.9
- key_gain: float32 [64], replicated, may hold values from 0.1 to 1.9
- key_bias: bfloat16 [6144, 16], P(('fs', 'sp'), 'tp'), parts along dimension 0, may hold values from -16 to 0
- eigen_real: float32 [64, 64], P('tp'), may hold values from -32 to 0
- eigen_imag: float32 [64, 64], P('tp'), may hold values from 0.31 to 201.0624
- log_step: float32 [64], P('tp'), may hold values from -6.91 to -2.3
- input_real: float32 [64, 64, 16], P('tp'), may hold values from -1 to 1
- input_imag: float32 [64, 64, 16], P('tp'), may hold values from -1 to 1
- read_real: float32 [64, 16, 64], P('tp'), may hold values from -0.75 to 0.75
- read_imag: float32 [64, 16, 64], P('tp'), may hold values from -0.75 to 0.75
- skip_gain: float32 [1024], P('tp'), may hold values from -6 to 6
- w_out_state: bfloat16 [1024, 2048], P('tp'), may hold values from -0.125 to 0.125
- w_out_attn: bfloat16 [1024, 2048], P('tp'), may hold values from -0.125 to 0.125
Outputs:
- layer_out: bfloat16 [6144, 2048], P(('fs', 'sp', 'tp')), parts along dimension 0
The draws below stay inside these ranges and needn't reach their ends.
There are 4 independent parts, one for each index of `fs`. The reference program is written for one: setup_inputs(seed, part) draws one part's arguments, and reference() takes and returns one part's arrays. A program takes and returns all parts, laid end to end along the dimension named above; an argument that names none is the same for every part. Nothing has to cross between parts.
All inputs are finite; a program needn't handle non-finite values.
Results may differ from the reference program's by a relative error of at most 0.014.
Values may be sent and summed in bfloat16 or wider, within the bound.
A program may use at most 128 MiB of HBM per device.

```python
import math
import jax
import jax.numpy as jnp
from jax import lax

D = 2048
GROUP = 16
GROUPS = 64
STATE = 64
HEADS = 16
HEAD_DIM = 64
TOK_DEV = 384
STATE_WIDTH = 1024
ATTN_WIDTH = 1024
SEQ = 1536
N_SP = 4
N_TP = 2


def draw_key_bias(key, part):
    rate_key, block_key, jitter_key, place_key, size_key = jax.random.split(jax.random.fold_in(key, 31), 5)
    ceiling = math.log(1.0 / 32.0)
    log_rates = jax.random.uniform(rate_key, (HEADS,), jnp.float32, math.log(0.05 / SEQ), ceiling)
    block_shift = jax.random.uniform(block_key, (SEQ // TOK_DEV, HEADS), jnp.float32, -0.7, 0.7)
    jitter = jax.random.uniform(jitter_key, (SEQ, HEADS), jnp.float32, -0.5, 0.5)
    reference_level = log_rates[None, :] + jnp.repeat(block_shift, TOK_DEV, axis=0) + jitter
    places = jax.random.randint(place_key, (3,), 0, SEQ)
    mixing_intensity = jax.random.uniform(size_key, (3, HEADS), jnp.float32, -1.4, -0.4)
    flagged_entries = (jnp.arange(SEQ)[:, None] == places[None, :]).astype(jnp.float32)
    tallied_count = jnp.sum(flagged_entries, axis=1, keepdims=True)
    spike_groups = jnp.dot(flagged_entries, mixing_intensity) / jnp.maximum(tallied_count, 1.0)
    return jnp.where(tallied_count > 0, spike_groups, reference_level).astype(jnp.bfloat16)


def state_rates(key):
    step_key, rate_key = jax.random.split(jax.random.fold_in(key, 47))
    log_step = jax.random.uniform(step_key, (GROUPS,), jnp.float32, math.log(0.001), math.log(0.1))
    ceiling = math.log(1.0 / 32.0)
    log_rates = jax.random.uniform(rate_key, (GROUPS, STATE), jnp.float32, math.log(0.05 / SEQ), ceiling)
    return (log_step, -jnp.exp(log_rates - log_step[:, None]))


def draw_eigen_real(key, part):
    return state_rates(key)[1]


def draw_log_step(key, part):
    return state_rates(key)[0]


def draw_eigen_imag(key, part):
    offsets = jax.random.uniform(jax.random.fold_in(key, 53), (GROUPS, STATE), jnp.float32, -0.4, 0.4)
    return math.pi * (jnp.arange(STATE, dtype=jnp.float32)[None, :] + 0.5 + offsets)


def steps_of(key, dims, pieces, low, high):
    factor_of = 1.0
    for axis_at, shards_of in pieces:
        draws = jax.random.uniform(jax.random.fold_in(jax.random.fold_in(key, 6), axis_at), (shards_of,), jnp.float32, low / len(pieces), high / len(pieces))
        factor_of = factor_of * jnp.repeat(jnp.exp(draws), dims[axis_at] // shards_of).reshape((-1,) + (1,) * (len(dims) - 1 - axis_at))
    return factor_of


def noise(stream_key, dims, scale, limit, cuts=(), kind=jnp.bfloat16):
    entries = jax.random.normal(stream_key, dims, jnp.float32) * scale
    if len(cuts) > 0:
        entries = steps_of(stream_key, dims, cuts, -0.22, 0.18) * entries
    return jnp.clip(entries, min=-limit, max=limit).astype(kind)


def setup_inputs(seed: int = 0, part: int = 0) -> dict:
    splits = jax.random.split(jax.random.key(seed), 20)
    part_splits = jax.random.split(jax.random.fold_in(splits[19], part), 20)
    return {
        "tokens": noise(part_splits[0], (SEQ, D), 1.0, 6.0, ((0, 8),)),
        "norm_gain": jnp.clip(1.0 + 0.18 * jax.random.normal(splits[1], (D,), jnp.float32), 0.1, 1.9),
        "w_input": noise(splits[2], (D, STATE_WIDTH), D ** -0.5, 0.125, ((1, 2),)),
        "w_query": noise(splits[3], (D, ATTN_WIDTH), D ** -0.5, 0.125, ((1, 2),)),
        "w_key": noise(splits[4], (D, ATTN_WIDTH), D ** -0.5, 0.125, ((1, 2),)),
        "w_value": noise(splits[5], (D, ATTN_WIDTH), D ** -0.5, 0.125, ((1, 2),)),
        "query_gain": jnp.clip(1.0 + 0.18 * jax.random.normal(splits[6], (HEAD_DIM,), jnp.float32), 0.1, 1.9),
        "key_gain": jnp.clip(1.0 + 0.18 * jax.random.normal(splits[7], (HEAD_DIM,), jnp.float32), 0.1, 1.9),
        "key_bias": draw_key_bias(jax.random.fold_in(jax.random.fold_in(splits[19], part), 71), part),
        "eigen_real": draw_eigen_real(jax.random.fold_in(splits[19], 71), part),
        "eigen_imag": draw_eigen_imag(jax.random.fold_in(splits[19], 71), part),
        "log_step": draw_log_step(jax.random.fold_in(splits[19], 71), part),
        "input_real": noise(splits[12], (GROUPS, STATE, GROUP), (2 * GROUP) ** -0.5, 1.0, ((0, 2),), jnp.float32),
        "input_imag": noise(splits[13], (GROUPS, STATE, GROUP), (2 * GROUP) ** -0.5, 1.0, ((0, 2),), jnp.float32),
        "read_real": noise(splits[14], (GROUPS, GROUP, STATE), STATE ** -0.5, 0.75, ((0, 2),), jnp.float32),
        "read_imag": noise(splits[15], (GROUPS, GROUP, STATE), STATE ** -0.5, 0.75, ((0, 2),), jnp.float32),
        "skip_gain": noise(splits[16], (STATE_WIDTH,), 1.0, 6.0, ((0, 2),), jnp.float32),
        "w_out_state": noise(splits[17], (STATE_WIDTH, D), (STATE_WIDTH + ATTN_WIDTH) ** -0.5, 0.125, ((0, 2),)),
        "w_out_attn": noise(splits[18], (ATTN_WIDTH, D), (STATE_WIDTH + ATTN_WIDTH) ** -0.5, 0.125, ((0, 2),)),
    }


EPSILON = 1e-06
PRECISE = lax.Precision.HIGHEST

def combine_states(earlier, later):
    leading_real_factor, first_ai, first_br, first_bi = earlier
    second_ar, second_ai, second_br, second_bi = later
    prod_r = second_ar * leading_real_factor - second_ai * first_ai
    prod_i = second_ar * first_ai + second_ai * leading_real_factor
    state_r = second_ar * first_br - second_ai * first_bi + second_br
    state_i = second_ar * first_bi + second_ai * first_br + second_bi
    return (prod_r, prod_i, state_r, state_i)

def discretize(eigen_real, eigen_imag, log_step, input_real, input_imag):
    step_size = jnp.exp(log_step)[:, None]
    rotation = eigen_imag * step_size
    shrink = jnp.expm1(eigen_real * step_size)
    cosine = jnp.cos(rotation)
    sine_part = jnp.sin(rotation)
    decay_r = (1.0 + shrink) * cosine
    decay_i = (1.0 + shrink) * sine_part
    minus_r = shrink * cosine - 2.0 * jnp.square(jnp.sin(0.5 * rotation))
    modulus = jnp.square(eigen_real) + jnp.square(eigen_imag)
    factor_r = (minus_r * eigen_real + decay_i * eigen_imag) / modulus
    factor_i = (decay_i * eigen_real - minus_r * eigen_imag) / modulus
    drive_r = factor_r[..., None] * input_real - factor_i[..., None] * input_imag
    drive_i = factor_r[..., None] * input_imag + factor_i[..., None] * input_real
    return (decay_r, decay_i, drive_r, drive_i)

def head_scale(flat_rows, head_gain):
    row_count = flat_rows.shape[0]
    shaped = flat_rows.astype(jnp.float32).reshape(row_count, HEADS, HEAD_DIM)
    scaled = shaped * lax.rsqrt(lax.optimization_barrier(jnp.mean(jnp.square(shaped), axis=-1, keepdims=True)) + EPSILON)
    return (scaled * head_gain).astype(jnp.bfloat16)

def block_terms(queries, key_rows, value_rows, bias_rows, q_first, k_first):
    scores = jnp.einsum('qhd,khd->hqk', queries.astype(jnp.float32), key_rows.astype(jnp.float32))
    scores = scores * HEAD_DIM ** (-0.5) + jnp.transpose(bias_rows.astype(jnp.float32))[:, None, :]
    query_place = q_first + jnp.arange(queries.shape[0], dtype=jnp.int32)
    key_place = k_first + jnp.arange(key_rows.shape[0], dtype=jnp.int32)
    causal = (key_place[None, :] < query_place[:, None])[None]
    log_keep = jnp.where(causal, jax.nn.log_sigmoid(-scores), 0.0)
    trailing_sum = lax.cumsum(log_keep, axis=2, reverse=True) - log_keep
    weights = jnp.where(causal, jnp.exp(jax.nn.log_sigmoid(scores) + trailing_sum), 0.0).astype(jnp.bfloat16)
    block_out = jnp.einsum('hqk,khd->qhd', weights.astype(jnp.float32), value_rows.astype(jnp.float32))
    return (block_out, lax.optimization_barrier(jnp.sum(log_keep, axis=2)))

def attention_branch(queries, key_heads, value_heads, key_bias):
    query_blocks = queries.reshape(N_SP, TOK_DEV, HEADS, HEAD_DIM)

    def one_query_block(operands):
        block_q, index = operands
        q_first = index * TOK_DEV

        def back_step(back_idx, carried):
            accumulated, later_sum = carried
            k_first = (index - back_idx) * TOK_DEV
            block_keys = lax.dynamic_slice_in_dim(key_heads, k_first, TOK_DEV, 0)
            block_values = lax.dynamic_slice_in_dim(value_heads, k_first, TOK_DEV, 0)
            block_bias = lax.dynamic_slice_in_dim(key_bias, k_first, TOK_DEV, 0)
            block_out, totals = block_terms(block_q, block_keys, block_values, block_bias, q_first, k_first)
            accumulated = accumulated + block_out * jnp.transpose(jnp.exp(later_sum))[:, :, None]
            return (accumulated, later_sum + totals)
        start_state = (jnp.zeros((TOK_DEV, HEADS, HEAD_DIM), jnp.float32), jnp.zeros((HEADS, TOK_DEV), jnp.float32))
        accumulated, _ = lax.fori_loop(0, index + 1, back_step, start_state)
        normed = accumulated * lax.rsqrt(lax.optimization_barrier(jnp.mean(jnp.square(accumulated), axis=-1, keepdims=True)) + EPSILON)
        return normed.astype(jnp.bfloat16)
    outputs = lax.map(one_query_block, (query_blocks, jnp.arange(N_SP, dtype=jnp.int32)))
    return outputs.reshape(SEQ, HEADS * HEAD_DIM)

def state_branch(inputs, eigen_real, eigen_imag, log_step, input_real, input_imag, read_real, read_imag, skip_gain):
    decay_r, decay_i, drive_r, drive_i = discretize(eigen_real, eigen_imag, log_step, input_real, input_imag)
    inputs_wide = inputs.astype(jnp.float32)
    grouped = jnp.transpose(inputs_wide.reshape(SEQ, GROUPS, GROUP), (1, 0, 2))

    def one_group(operands):
        group_in, dec_r, dec_i, drv_r, drv_i, rd_r, rd_i = operands
        push_r = jnp.dot(group_in, jnp.transpose(drv_r), precision=PRECISE, preferred_element_type=jnp.float32)
        push_i = jnp.dot(group_in, jnp.transpose(drv_i), precision=PRECISE, preferred_element_type=jnp.float32)
        steps_r = jnp.broadcast_to(dec_r[None, :], push_r.shape)
        steps_i = jnp.broadcast_to(dec_i[None, :], push_i.shape)
        running = lax.associative_scan(combine_states, (steps_r, steps_i, push_r, push_i), axis=0)
        real_read = jnp.dot(running[2], jnp.transpose(rd_r), precision=PRECISE, preferred_element_type=jnp.float32)
        imag_read = jnp.dot(running[3], jnp.transpose(rd_i), precision=PRECISE, preferred_element_type=jnp.float32)
        return real_read - imag_read
    outputs = lax.map(one_group, (grouped, decay_r, decay_i, drive_r, drive_i, read_real, read_imag))
    readout = jnp.transpose(outputs, (1, 0, 2)).reshape(SEQ, GROUPS * GROUP)
    return jax.nn.gelu(readout + skip_gain * inputs_wide).astype(jnp.bfloat16)

def reference(tokens, norm_gain, w_input, w_query, w_key, w_value, query_gain, key_gain, key_bias, eigen_real, eigen_imag, log_step, input_real, input_imag, read_real, read_imag, skip_gain, w_out_state, w_out_attn):
    token_rows = tokens.astype(jnp.float32)
    scale_rows = lax.rsqrt(lax.optimization_barrier(jnp.mean(jnp.square(token_rows), axis=-1, keepdims=True)) + EPSILON)
    normed = (token_rows * scale_rows * norm_gain).astype(jnp.bfloat16)
    inputs = jnp.dot(normed, w_input, preferred_element_type=jnp.float32).astype(jnp.bfloat16)
    query_rows = jnp.dot(normed, w_query, preferred_element_type=jnp.float32).astype(jnp.bfloat16)
    key_rows = jnp.dot(normed, w_key, preferred_element_type=jnp.float32).astype(jnp.bfloat16)
    value_rows = jnp.dot(normed, w_value, preferred_element_type=jnp.float32).astype(jnp.bfloat16)
    queries = head_scale(query_rows, query_gain)
    key_heads = head_scale(key_rows, key_gain)
    value_heads = value_rows.reshape(SEQ, HEADS, HEAD_DIM)
    attn_out = attention_branch(queries, key_heads, value_heads, key_bias)
    state_out = state_branch(inputs, eigen_real, eigen_imag, log_step, input_real, input_imag, read_real, read_imag, skip_gain)
    state_cols = STATE_WIDTH // N_TP
    attn_cols = ATTN_WIDTH // N_TP

    def add_term(index, summed):
        state_part = lax.dynamic_slice_in_dim(state_out, index * state_cols, state_cols, 1)
        attn_part = lax.dynamic_slice_in_dim(attn_out, index * attn_cols, attn_cols, 1)
        state_weight = lax.dynamic_slice_in_dim(w_out_state, index * state_cols, state_cols, 0)
        attn_weight = lax.dynamic_slice_in_dim(w_out_attn, index * attn_cols, attn_cols, 0)
        term = jnp.dot(state_part, state_weight, preferred_element_type=jnp.float32)
        term = term + jnp.dot(attn_part, attn_weight, preferred_element_type=jnp.float32)
        term = lax.optimization_barrier(term.astype(jnp.bfloat16)).astype(jnp.float32)
        return summed + term
    summed = lax.fori_loop(0, N_TP, add_term, jnp.zeros((SEQ, D), jnp.float32))
    return summed.astype(jnp.bfloat16)
```

```python
import functools

import jax
import jax.numpy as jnp
from jax import lax
from jax.experimental import pallas as pl
from jax.experimental.pallas import tpu as pltpu
from jax.sharding import PartitionSpec as P

GROUP = 16
STATE = 64
HEAD_DIM = 64


EPSILON = 1e-06
PRECISE = lax.Precision.HIGHEST


def from_behind(block, axis, distance):
    devices = range(lax.axis_size(axis))
    route = [(i - distance, i) for i in devices if i - distance in devices]
    return lax.ppermute(block, axis, route)


def carried_in(part, axis, combine, identity):
    place = lax.axis_index(axis)
    gathered = jax.tree.map(lambda a: lax.all_gather(a, axis), part)
    state = jax.tree.map(lambda a, e: jnp.zeros_like(a) + jnp.asarray(e, a.dtype), part, identity)

    def one(lap, state):
        return combine(
            state, jax.tree.map(lambda a: lax.dynamic_index_in_dim(a, lap, 0, False), gathered)
        )

    return lax.fori_loop(0, place, one, state)


def combine_states(earlier, later):
    leading_real_factor, first_ai, first_br, first_bi = earlier
    second_ar, second_ai, second_br, second_bi = later
    prod_r = second_ar * leading_real_factor - second_ai * first_ai
    prod_i = second_ar * first_ai + second_ai * leading_real_factor
    state_r = second_ar * first_br - second_ai * first_bi + second_br
    state_i = second_ar * first_bi + second_ai * first_br + second_bi
    return (prod_r, prod_i, state_r, state_i)


def discretize(eigen_real, eigen_imag, log_step, input_real, input_imag):
    step_size = jnp.exp(log_step)[:, None]
    rotation = eigen_imag * step_size
    shrink = jnp.expm1(eigen_real * step_size)
    cosine = jnp.cos(rotation)
    sine_part = jnp.sin(rotation)
    decay_r = (1.0 + shrink) * cosine
    decay_i = (1.0 + shrink) * sine_part
    minus_r = shrink * cosine - 2.0 * jnp.square(jnp.sin(0.5 * rotation))
    modulus = jnp.square(eigen_real) + jnp.square(eigen_imag)
    factor_r = (minus_r * eigen_real + decay_i * eigen_imag) / modulus
    factor_i = (decay_i * eigen_real - minus_r * eigen_imag) / modulus
    drive_r = factor_r[..., None] * input_real - factor_i[..., None] * input_imag
    drive_i = factor_r[..., None] * input_imag + factor_i[..., None] * input_real
    return (decay_r, decay_i, drive_r, drive_i)


def head_scale(flat_rows, head_gain, head_count):
    row_count = flat_rows.shape[0]
    shaped = flat_rows.astype(jnp.float32).reshape(row_count, head_count, HEAD_DIM)
    scaled = shaped * lax.rsqrt(jnp.mean(jnp.square(shaped), axis=-1, keepdims=True) + EPSILON)
    return (scaled * head_gain).astype(jnp.bfloat16)


def block_terms(queries, key_rows, value_rows, bias_rows, q_first, k_first):
    head_count = queries.shape[1]
    key_heads = key_rows.reshape(key_rows.shape[0], head_count, HEAD_DIM)
    value_heads = value_rows.reshape(value_rows.shape[0], head_count, HEAD_DIM)
    scores = jnp.einsum("qhd,khd->hqk", queries, key_heads, preferred_element_type=jnp.float32)
    scores = scores * HEAD_DIM ** (-0.5) + jnp.transpose(bias_rows.astype(jnp.float32))[:, None, :]
    query_place = q_first + lax.iota(jnp.int32, queries.shape[0])
    key_place = k_first + lax.iota(jnp.int32, key_rows.shape[0])
    causal = (key_place[None, :] < query_place[:, None])[None]
    log_keep = jnp.where(causal, jax.nn.log_sigmoid(-scores), 0.0)
    trailing_sum = lax.cumsum(log_keep, axis=2, reverse=True) - log_keep
    weights = jnp.where(causal, jnp.exp(jax.nn.log_sigmoid(scores) + trailing_sum), 0.0).astype(
        jnp.bfloat16
    )
    block_out = jnp.einsum("hqk,khd->qhd", weights, value_heads, preferred_element_type=jnp.float32)
    return (block_out.reshape(queries.shape[0], head_count * HEAD_DIM), jnp.sum(log_keep, axis=2))


def guarded_terms(queries, key_rows, value_rows, bias_rows, q_first, k_first):
    live = jnp.logical_and(k_first >= 0, k_first <= q_first)

    def compute_block():
        return block_terms(queries, key_rows, value_rows, bias_rows, q_first, k_first)

    def empty_block():
        return (
            jnp.zeros((queries.shape[0], queries.shape[1] * HEAD_DIM), jnp.float32),
            jnp.zeros((queries.shape[1], queries.shape[0]), jnp.float32),
        )

    return lax.cond(live, compute_block, empty_block)


def merge_blocks(block_parts, totals):
    blocks, row_count, row_width = block_parts.shape
    head_count = totals.shape[1]
    later_sum = jnp.flip(jnp.cumsum(jnp.flip(totals, 0), axis=0), 0) - totals
    factors = jnp.exp(jnp.transpose(later_sum, (0, 2, 1)))[..., None]

    def add_block(block_idx, accumulated):
        part = lax.dynamic_index_in_dim(block_parts, block_idx, 0, keepdims=False)
        factor = lax.dynamic_index_in_dim(factors, block_idx, 0, keepdims=False)
        return accumulated + part.reshape(row_count, head_count, HEAD_DIM) * factor

    accumulated = lax.fori_loop(
        0, blocks, add_block, jnp.zeros((row_count, head_count, HEAD_DIM), jnp.float32)
    )
    normed = accumulated * lax.rsqrt(
        jnp.mean(jnp.square(accumulated), axis=-1, keepdims=True) + EPSILON
    )
    return normed.reshape(row_count, row_width).astype(jnp.bfloat16)


def attend(queries, key_rows, value_rows, bias_rows):
    row_count = queries.shape[0]
    head_count = queries.shape[1]
    row_width = key_rows.shape[1]
    my_first = lax.axis_index("sp") * row_count
    levels = (lax.axis_size("sp") - 1).bit_length()
    slot_count = 2**levels
    own_out, own_totals = block_terms(queries, key_rows, value_rows, bias_rows, my_first, my_first)
    block_parts = lax.dynamic_update_slice_in_dim(
        jnp.zeros((slot_count, row_count, row_width), jnp.float32), own_out[None], 0, 0
    )
    totals = lax.dynamic_update_slice_in_dim(
        jnp.zeros((slot_count, head_count, row_count), jnp.float32), own_totals[None], 0, 0
    )
    held_keys = (key_rows, value_rows, bias_rows)
    for level_idx in range(levels):
        distance_base = 2**level_idx
        arrived = from_behind((held_keys[0], held_keys[1], held_keys[2]), "sp", distance_base)

        def one_block(inner_idx, current, arrived=arrived, distance_base=distance_base):
            offset = inner_idx * row_count
            distance = distance_base + inner_idx
            k_first = my_first - distance * row_count
            block_out, block_totals = guarded_terms(
                queries,
                lax.dynamic_slice_in_dim(arrived[0], offset, row_count, 0),
                lax.dynamic_slice_in_dim(arrived[1], offset, row_count, 0),
                lax.dynamic_slice_in_dim(arrived[2], offset, row_count, 0),
                my_first,
                k_first,
            )
            return (
                lax.dynamic_update_slice_in_dim(current[0], block_out[None], distance, 0),
                lax.dynamic_update_slice_in_dim(current[1], block_totals[None], distance, 0),
            )

        block_parts, totals = lax.fori_loop(0, distance_base, one_block, (block_parts, totals))
        if level_idx + 1 < levels:
            held_keys = (
                jnp.concatenate([held_keys[0], arrived[0]], axis=0),
                jnp.concatenate([held_keys[1], arrived[1]], axis=0),
                jnp.concatenate([held_keys[2], arrived[2]], axis=0),
            )
    return merge_blocks(jnp.flip(block_parts, 0), jnp.flip(totals, 0))


def state_branch(
    inputs,
    eigen_real,
    eigen_imag,
    log_step,
    input_real,
    input_imag,
    read_real,
    read_imag,
    skip_gain,
):
    decay_r, decay_i, drive_r, drive_i = discretize(
        eigen_real, eigen_imag, log_step, input_real, input_imag
    )
    row_count = inputs.shape[0]
    groups = eigen_real.shape[0]
    inputs_wide = inputs.astype(jnp.float32)
    grouped = inputs_wide.reshape(row_count, groups, GROUP)
    push_r = jnp.einsum("lgh,gph->lgp", grouped, drive_r, precision=PRECISE).reshape(
        row_count, groups * STATE
    )
    push_i = jnp.einsum("lgh,gph->lgp", grouped, drive_i, precision=PRECISE).reshape(
        row_count, groups * STATE
    )
    steps_r = jnp.broadcast_to(decay_r.reshape(1, groups * STATE), push_r.shape)
    steps_i = jnp.broadcast_to(decay_i.reshape(1, groups * STATE), push_i.shape)
    running = lax.associative_scan(combine_states, (steps_r, steps_i, push_r, push_i), axis=0)
    block_ends = (
        running[0][row_count - 1],
        running[1][row_count - 1],
        running[2][row_count - 1],
        running[3][row_count - 1],
    )
    identity = (
        jnp.ones((groups * STATE,), jnp.float32),
        jnp.zeros((groups * STATE,), jnp.float32),
        jnp.zeros((groups * STATE,), jnp.float32),
        jnp.zeros((groups * STATE,), jnp.float32),
    )
    before = carried_in(block_ends, "sp", combine_states, identity)
    state_r = running[2] + running[0] * before[2][None, :] - running[1] * before[3][None, :]
    state_i = running[3] + running[0] * before[3][None, :] + running[1] * before[2][None, :]
    readout = jnp.einsum(
        "lgp,ghp->lgh", state_r.reshape(row_count, groups, STATE), read_real, precision=PRECISE
    )
    readout = readout - jnp.einsum(
        "lgp,ghp->lgh", state_i.reshape(row_count, groups, STATE), read_imag, precision=PRECISE
    )
    mixed = readout.reshape(row_count, groups * GROUP) + skip_gain * inputs_wide
    return jax.nn.gelu(mixed).astype(jnp.bfloat16)


def plain_device(
    tokens,
    norm_gain,
    w_input,
    w_query,
    w_key,
    w_value,
    query_gain,
    key_gain,
    key_bias,
    eigen_real,
    eigen_imag,
    log_step,
    input_real,
    input_imag,
    read_real,
    read_imag,
    skip_gain,
    w_out_state,
    w_out_attn,
):
    token_rows = tokens.astype(jnp.float32)
    scale_rows = lax.rsqrt(jnp.mean(jnp.square(token_rows), axis=-1, keepdims=True) + EPSILON)
    normed = (token_rows * scale_rows * norm_gain).astype(jnp.bfloat16)
    w_joined = jnp.concatenate([w_input, w_query, w_key, w_value], axis=1)
    projected = jnp.dot(
        lax.all_gather(normed, "tp", axis=0, tiled=True),
        w_joined,
        preferred_element_type=jnp.float32,
    ).astype(jnp.bfloat16)
    state_width = w_input.shape[1]
    attn_width = w_query.shape[1]
    head_count = attn_width // HEAD_DIM
    inputs = projected[:, :state_width]
    query_rows = projected[:, state_width : state_width + attn_width]
    key_rows = projected[:, state_width + attn_width : state_width + 2 * attn_width]
    value_rows = projected[:, state_width + 2 * attn_width :]
    queries = head_scale(query_rows, query_gain, head_count)
    key_normed = head_scale(key_rows, key_gain, head_count).reshape(key_rows.shape[0], attn_width)
    attn_out = attend(queries, key_normed, value_rows, key_bias)
    state_out = state_branch(
        inputs,
        eigen_real,
        eigen_imag,
        log_step,
        input_real,
        input_imag,
        read_real,
        read_imag,
        skip_gain,
    )
    summed_part = jnp.dot(state_out, w_out_state, preferred_element_type=jnp.float32)
    return lax.psum_scatter(
        (summed_part + jnp.dot(attn_out, w_out_attn, preferred_element_type=jnp.float32)).astype(
            jnp.bfloat16
        ),
        "tp",
        scatter_dimension=0,
        tiled=True,
    )


LANES = 128
NT = (((1,), (1,)), ((), ()))


def dot_nt(a, b):
    return lax.dot_general(a, b, NT, preferred_element_type=jnp.float32)


def dot_nn(a, b):
    return jnp.dot(a, b, preferred_element_type=jnp.float32)


def by_head(low, high, shape):
    return jnp.where(lax.broadcasted_iota(jnp.int32, shape, 1) < HEAD_DIM, low, high)


def head_rms(rows):
    square = rows * rows
    low = jnp.sum(by_head(square, 0.0, rows.shape), axis=-1, keepdims=True)
    high = jnp.sum(by_head(0.0, square, rows.shape), axis=-1, keepdims=True)
    mean = by_head(low, high, rows.shape) * (1.0 / HEAD_DIM)
    return rows * lax.rsqrt(mean + EPSILON)


def complex_power(real, imag, exponent):
    out_r, out_i = None, None
    while exponent:
        if exponent & 1:
            if out_r is None:
                out_r, out_i = real, imag
            else:
                out_r, out_i = out_r * real - out_i * imag, out_r * imag + out_i * real
        exponent >>= 1
        if exponent:
            real, imag = real * real - imag * imag, 2.0 * real * imag
    return out_r, out_i


LOG2E = 1.4426950408889634
OWNERS = (0, 1, 1, 2)


def owned_span(owner):
    held = [pair for pair, rank in enumerate(OWNERS) if rank == owner]
    return (held[0], held[-1] + 1) if held else (0, 0)


def routes():
    early, late, onward = [], [], []
    for kind in ("k", "v"):
        early.append((kind, 0, 1, 0, owned_span(2)))
        early.append((kind, 1, 2, 1, owned_span(2)))
        early.append((kind, 1, 0, 1, owned_span(0)))
        early.append((kind, 2, 3, 0, (0, len(OWNERS))))
        late.append((kind, 0, 1, 0, owned_span(1)))
        late.append((kind, 0, 1, 0, owned_span(0)))
        onward.append((kind, 1, 2, 0, owned_span(2)))
    for slot in range(2):
        for owner in range(3):
            if owner != slot + 2:
                early.append(("q", slot + 2, owner, slot, owned_span(owner)))
    biases = [("b", 0, 1, 0), ("b", 1, 0, 1), ("b", 0, 2, 0), ("b", 1, 2, 1), ("b", 2, 3, 0)]
    keep = [[route for route in group if route[4][0] < route[4][1]] for group in (early, late, onward)]
    return keep[0], keep[1], keep[2], biases


def route_count():
    early, late, onward, biases = routes()
    return 2 * len(early) + len(late) + len(onward) + len(biases)


def mixer_kernel(
    ranks,
    tokens_ref,
    norm_gain_ref,
    w_input_ref,
    w_query_ref,
    w_key_ref,
    w_value_ref,
    w_state_ref,
    w_attn_ref,
    q_gain_ref,
    k_gain_ref,
    bias_ref,
    decay_r_ref,
    decay_i_ref,
    factor_r_ref,
    factor_i_ref,
    input_r_ref,
    input_i_ref,
    read_r_ref,
    read_i_ref,
    skip_ref,
    out_ref,
    normed,
    decay_ref,
    state_part,
    w_held,
    w_out,
    act_ref,
    u_ref,
    v_ref,
    q_norm,
    k_norm,
    bias_stage,
    out_part,
    out_arrived,
    w_sem,
    row_sem,
    part_send,
    part_recv,
    q_far,
    k_far,
    v_far,
    bias_far,
    push_r,
    push_i,
    up_ref,
    seg_r,
    seg_i,
    ends_land,
    acc_own,
    run_own,
    acc_far,
    run_far,
    far_stage,
    far_land,
    route_send,
    route_recv,
    end_send,
    end_recv,
    back_send,
    back_recv,
):
    rows, width = u_ref.shape
    states = decay_ref.shape[1]
    chunks = rows // LANES
    pairs = width // LANES
    seg_len = rows // 8
    own_count, features = tokens_ref.shape
    core = lax.axis_index("tp")
    own_rows = pl.ds(pl.multiple_of(core * own_count, own_count), own_count)
    mate_rows = pl.ds(pl.multiple_of((1 - core) * own_count, own_count), own_count)
    mate = {"device_id": {"tp": 1 - core}, "device_id_type": pl.DeviceIdType.MESH}
    halves = width // 256
    span = states // halves
    me = lax.axis_index("sp")
    others = range(1, ranks)

    def at_rank(step):
        return lax.rem(me + step, ranks)

    barrier = pltpu.get_barrier_semaphore()
    for step in others:
        pl.semaphore_signal(
            barrier, inc=1, device_id={"sp": at_rank(step)}, device_id_type=pl.DeviceIdType.MESH
        )

    pl.semaphore_signal(barrier, inc=1, **mate)
    weights = []
    for slot, ref in enumerate((w_key_ref, w_value_ref, w_query_ref, w_input_ref)):
        weights.append(pltpu.make_async_copy(ref, w_held.at[slot], w_sem.at[slot]))
    for slot, ref in enumerate((w_state_ref, w_attn_ref)):
        target = w_out.at[slot * width : (slot + 1) * width, :]
        weights.append(pltpu.make_async_copy(ref, target, w_sem.at[4 + slot]))
    for copy in weights:
        copy.start()

    token_rows = tokens_ref[...].astype(jnp.float32)
    mean = jnp.sum(token_rows * token_rows, axis=-1, keepdims=True) * (1.0 / features)
    scaled = token_rows * lax.rsqrt(mean + EPSILON) * norm_gain_ref[...]
    normed[own_rows, :] = scaled.astype(jnp.bfloat16)
    bias = bias_ref[...].astype(jnp.float32) * LOG2E
    for chunk in range(chunks):
        for head in range(2 * pairs):
            lanes = slice((head % 2) * LANES, (head % 2 + 1) * LANES)
            bias_stage[chunk, head // 2 : head // 2 + 1, lanes] = bias[
                head : head + 1, chunk * LANES : (chunk + 1) * LANES
            ]
    q_gain, k_gain = (
        jnp.concatenate([ref[...], ref[...]], axis=1) for ref in (q_gain_ref, k_gain_ref)
    )
    q_gain = q_gain * (LOG2E * HEAD_DIM**-0.5)
    groups = decay_r_ref.shape[0]
    for row, ref in enumerate((decay_r_ref, decay_i_ref)):
        decay_ref[row : row + 1, :] = jnp.concatenate(
            [ref[group : group + 1, :] for group in range(groups)], axis=1
        )

    early, late, onward, biases = routes()
    sources = {"q": q_norm, "k": k_norm, "v": v_ref}
    targets = {"q": q_far, "k": k_far, "v": v_far}
    issued = []

    def make_route(ident, route, at, relay=False):
        kind, origin, goal, slot = route[:4]
        if kind == "b":
            source, target = bias_stage, bias_far.at[slot]
        else:
            cols = slice(route[4][0] * LANES, route[4][1] * LANES)
            target = targets[kind].at[slot, at, cols]
            source = target if relay else sources[kind].at[at, cols]
        return pltpu.make_async_remote_copy(
            src_ref=source,
            dst_ref=target,
            send_sem=route_send.at[ident],
            recv_sem=route_recv.at[ident],
            device_id={"sp": goal},
            device_id_type=pl.DeviceIdType.MESH,
        )

    def start_routes(chosen, at, relay=False):
        entries = []
        for route in chosen:
            entries.append((len(issued), route, make_route(len(issued), route, at, relay)))
            issued.append((route, entries[-1][2]))
        for origin in range(ranks):
            sent = [copy for _, route, copy in entries if route[1] == origin]
            if sent:

                @pl.when(me == origin)
                def _(sent=sent):
                    for copy in sent:
                        copy.start()

    waited = set()

    def wait_routes(test):
        for goal in range(ranks):
            due = [
                index
                for index, (route, _) in enumerate(issued)
                if route[2] == goal and index not in waited and test(route)
            ]
            waited.update(due)
            if due:

                @pl.when(me == goal)
                def _(due=due):
                    for index in due:
                        issued[index][1].wait_recv()

    pl.semaphore_wait(barrier, ranks)
    row_copy = pltpu.make_async_remote_copy(
        src_ref=normed.at[own_rows, :],
        dst_ref=normed.at[own_rows, :],
        send_sem=row_sem.at[0],
        recv_sem=row_sem.at[1],
        **mate,
    )
    row_copy.start()
    start_routes(biases, None)

    def project(slot, at):
        flat = dot_nn(normed[at, :], w_held[slot]).astype(jnp.bfloat16)
        if slot == 1:
            v_ref[at, :] = flat
        elif slot == 3:
            u_ref[at, :] = flat
        else:
            gain, target = (k_gain, k_norm) if slot == 0 else (q_gain, q_norm)
            for tile in range(width // LANES):
                cols = slice(tile * LANES, (tile + 1) * LANES)
                part = head_rms(flat[:, cols].astype(jnp.float32)) * gain
                target[at, cols] = part.astype(jnp.bfloat16)

    for slot, kind in enumerate("kvq"):
        weights[slot].wait()
        project(slot, own_rows)
        start_routes([route for route in early if route[0] == kind], own_rows)
    row_copy.wait_recv()
    for slot, kind in enumerate("kvq"):
        project(slot, mate_rows)
        start_routes([route for route in early if route[0] == kind], mate_rows)
    whole = slice(0, rows)
    start_routes(late, whole)
    weights[3].wait()
    project(3, whole)

    def place(axis):
        index = lax.broadcasted_iota(jnp.int32, (rows, rows), axis)
        other = lax.broadcasted_iota(jnp.int32, (rows, rows), 1 - axis)
        return jnp.where(other == (index & 7) * seg_len + (index >> 3), 1.0, 0.0).astype(
            jnp.bfloat16
        )

    up_ref[...] = dot_nn(place(0), u_ref[...]).astype(jnp.bfloat16)

    spread_state = lax.broadcasted_iota(jnp.int32, (STATE, span), 0) == (
        lax.broadcasted_iota(jnp.int32, (STATE, span), 1) & (STATE - 1)
    )
    spread_state = jnp.where(spread_state, 1.0, 0.0).astype(jnp.bfloat16)

    def by_channel(ref):
        wide = jnp.broadcast_to(ref[...][:, None, :], (groups, GROUP, STATE))
        return wide.reshape(groups * GROUP, STATE)

    factor_r = by_channel(factor_r_ref)
    factor_i = by_channel(factor_i_ref)
    drive_r = factor_r * input_r_ref[...] - factor_i * input_i_ref[...]
    drive_i = factor_r * input_i_ref[...] + factor_i * input_r_ref[...]

    def block_diagonal(values, half):
        row_group = lax.broadcasted_iota(jnp.int32, (256, span), 0) // GROUP
        col_group = lax.broadcasted_iota(jnp.int32, (256, span), 1) // STATE
        wide = dot_nn(
            values[half * 256 : (half + 1) * 256, :].astype(jnp.bfloat16), spread_state
        )
        return jnp.where(row_group == col_group, wide, 0.0).astype(jnp.bfloat16)

    for half in range(halves):
        cols = slice(half * span, (half + 1) * span)
        part = up_ref[:, half * 256 : (half + 1) * 256]
        push_r[:, cols] = dot_nn(part, block_diagonal(drive_r, half))
        push_i[:, cols] = dot_nn(part, block_diagonal(drive_i, half))

    block = 512

    def scan(keep_states):
        for first in range(0, states, block):
            cols = slice(first, first + block)
            step_r = jnp.broadcast_to(decay_ref[0:1, cols], (8, block))
            step_i = jnp.broadcast_to(decay_ref[1:2, cols], (8, block))

            def one(index, state, cols=cols, step_r=step_r, step_i=step_i):
                state_r, state_i = state
                at = pl.ds(pl.multiple_of(index * 8, 8), 8)
                next_r = step_r * state_r - step_i * state_i + push_r[at, cols]
                next_i = step_r * state_i + step_i * state_r + push_i[at, cols]
                if keep_states:
                    push_r[at, cols] = next_r
                    push_i[at, cols] = next_i
                return (next_r, next_i)

            if keep_states:
                start = (seg_r[:, cols], seg_i[:, cols])
            else:
                start = (jnp.zeros((8, block), jnp.float32),) * 2
            state_r, state_i = lax.fori_loop(0, seg_len, one, start, unroll=4)
            if not keep_states:
                seg_r[:, cols] = state_r
                seg_i[:, cols] = state_i

    scan(False)
    seg_step_r, seg_step_i = complex_power(decay_ref[0:1, :], decay_ref[1:2, :], seg_len)
    end_r = jnp.zeros((1, states), jnp.float32)
    end_i = jnp.zeros((1, states), jnp.float32)
    for seg in range(8):
        end_r, end_i = (
            seg_step_r * end_r - seg_step_i * end_i + seg_r[seg : seg + 1, :],
            seg_step_r * end_i + seg_step_i * end_r + seg_i[seg : seg + 1, :],
        )
    ends_land[me, 0:1, :] = end_r
    ends_land[me, 1:2, :] = end_i
    end_copies = []
    for step in others:
        copy = pltpu.make_async_remote_copy(
            src_ref=ends_land.at[me],
            dst_ref=ends_land.at[me],
            send_sem=end_send.at[step],
            recv_sem=end_recv.at[step],
            device_id={"sp": at_rank(step)},
            device_id_type=pl.DeviceIdType.MESH,
        )
        copy.start()
        end_copies.append(copy)

    tail = lax.broadcasted_iota(jnp.int32, (2 * LANES, 2 * LANES), 0)
    col = lax.broadcasted_iota(jnp.int32, (2 * LANES, 2 * LANES), 1)
    tail = jnp.where(
        jnp.logical_and(tail >= col, tail // LANES == col // LANES), 1.0, 0.0
    ).astype(jnp.bfloat16)
    lane = lax.broadcasted_iota(jnp.int32, (1, LANES), 1)
    low_mask = jnp.where(lane < HEAD_DIM, 1.0, 0.0).astype(jnp.bfloat16)
    high_mask = jnp.where(lane < HEAD_DIM, 0.0, 1.0).astype(jnp.bfloat16)

    def both_heads(block):
        return jnp.concatenate([block * low_mask, block * high_mask], axis=0)

    def attend(queries, keys, values, bias_row, running, diagonal):
        count = queries.shape[0]
        z = dot_nt(queries, both_heads(keys)) + bias_row
        soft = jnp.log(1.0 + jnp.exp2(z)) * LOG2E
        if diagonal:
            causal = (lax.broadcasted_iota(jnp.int32, z.shape, 1) & (LANES - 1)) < (
                lax.broadcasted_iota(jnp.int32, z.shape, 0)
            )
            soft = jnp.where(causal, soft, 0.0)
        sums = dot_nn(soft.astype(jnp.bfloat16), tail)
        weight = jnp.exp2(z - (sums + running))
        if diagonal:
            weight = jnp.where(causal, weight, 0.0)
        totals = jnp.concatenate(
            [
                jnp.broadcast_to(sums[:, :1], (count, LANES)),
                jnp.broadcast_to(sums[:, LANES : LANES + 1], (count, LANES)),
            ],
            axis=1,
        )
        part = dot_nn(weight.astype(jnp.bfloat16), both_heads(values))
        return part, running + totals

    def pair_cols(pair):
        return pl.ds(pl.multiple_of(pair * LANES, LANES), LANES)

    def run_cols(pair):
        return pl.ds(pl.multiple_of(pair * 2 * LANES, 2 * LANES), 2 * LANES)

    def own_pair(pair, carry):
        cols, wide = pair_cols(pair), run_cols(pair)
        acc_own[:, cols] = jnp.zeros((rows, LANES), jnp.float32)
        run_own[:, wide] = jnp.zeros((rows, 2 * LANES), jnp.float32)
        for chunk in reversed(range(chunks)):
            at = slice(chunk * LANES, (chunk + 1) * LANES)
            below = slice(chunk * LANES, rows)
            part, running = attend(
                q_norm[below, cols],
                k_norm[at, cols],
                v_ref[at, cols],
                bias_stage[chunk, pl.ds(pair, 1), :],
                run_own[below, wide],
                True,
            )
            acc_own[below, cols] += part
            run_own[below, wide] = running
        return carry

    def near_pair(pair, carry):
        cols, wide = pair_cols(pair), run_cols(pair)
        for chunk in reversed(range(chunks)):
            at = slice(chunk * LANES, (chunk + 1) * LANES)
            part, running = attend(
                q_norm[:, cols],
                k_far[0, at, cols],
                v_far[0, at, cols],
                bias_far[0, chunk, pl.ds(pair, 1), :],
                run_own[:, wide],
                False,
            )
            acc_own[:, cols] += part
            run_own[:, wide] = running
        return carry

    def far_copy(slot, pair):
        return pltpu.make_async_remote_copy(
            src_ref=far_stage.at[slot, :, pair_cols(pair)],
            dst_ref=far_land.at[:, pair_cols(pair)],
            send_sem=back_send.at[slot, pair],
            recv_sem=back_recv.at[pair],
            device_id={"sp": slot + 2},
            device_id_type=pl.DeviceIdType.MESH,
        )

    def far_pair(pair, carry):
        cols = pair_cols(pair)
        queries = q_far[:, :, cols].reshape(2 * rows, LANES)
        acc_far[...] = jnp.zeros_like(acc_far)
        run_far[...] = jnp.zeros_like(run_far)

        def key_block(step, inner):
            slot = 1 - step
            for chunk in reversed(range(chunks)):
                at = slice(chunk * LANES, (chunk + 1) * LANES)
                part, running = attend(
                    queries,
                    k_far[slot, at, cols],
                    v_far[slot, at, cols],
                    bias_far[slot, chunk, pl.ds(pair, 1), :],
                    run_far[...],
                    False,
                )
                acc_far[...] += part
                run_far[...] = running
            return inner

        lax.fori_loop(0, 2, key_block, 0)
        for slot in range(2):
            part = acc_far[slot * rows : (slot + 1) * rows, :].astype(jnp.bfloat16)

            @pl.when(me == slot + 2)
            def _(part=part):
                far_land[:, cols] = part

            @pl.when(me != slot + 2)
            def _(part=part, slot=slot):
                far_stage[slot, :, cols] = part
                far_copy(slot, pair).start()

        return carry

    first_pair, last_pair = jnp.int32(0), jnp.int32(0)
    for owner in range(3):
        first_pair = jnp.where(me == owner, owned_span(owner)[0], first_pair)
        last_pair = jnp.where(me == owner, owned_span(owner)[1], last_pair)

    if onward:
        wait_routes(lambda route: route[2] == 1 and route[0] in "kv" and route[4] == owned_span(2))
        start_routes(onward, whole, True)
    lax.fori_loop(0, pairs, own_pair, 0)
    for owner, (slot, held, kept) in enumerate(
        (
            (0, ((k_norm, k_far), (v_ref, v_far), (bias_stage, bias_far)), None),
            (1, ((k_norm, k_far), (v_ref, v_far), (bias_stage, bias_far)), None),
            (0, ((q_norm, q_far),), None),
        )
    ):
        @pl.when(me == owner)
        def _(slot=slot, held=held):
            for source, target in held:
                target[slot] = source[...]

    wait_routes(lambda route: route[2] < 3)
    lax.fori_loop(first_pair, last_pair, far_pair, 0)
    wait_routes(lambda route: True)

    @pl.when(lax.rem(me, 2) == 1)
    def _():
        lax.fori_loop(0, pairs, near_pair, 0)

    for copy in end_copies:
        copy.wait_recv()
    block_r, block_i = complex_power(decay_ref[0:1, :], decay_ref[1:2, :], rows)
    carry_r = jnp.zeros((1, states), jnp.float32)
    carry_i = jnp.zeros((1, states), jnp.float32)
    for rank in range(ranks - 1):
        next_r = block_r * carry_r - block_i * carry_i + ends_land[rank, 0:1, :]
        next_i = block_r * carry_i + block_i * carry_r + ends_land[rank, 1:2, :]
        carry_r = jnp.where(rank < me, next_r, carry_r)
        carry_i = jnp.where(rank < me, next_i, carry_i)
    for seg in range(8):
        own_r = seg_r[seg : seg + 1, :]
        own_i = seg_i[seg : seg + 1, :]
        seg_r[seg : seg + 1, :] = carry_r
        seg_i[seg : seg + 1, :] = carry_i
        carry_r, carry_i = (
            seg_step_r * carry_r - seg_step_i * carry_i + own_r,
            seg_step_r * carry_i + seg_step_i * carry_r + own_i,
        )
    scan(True)

    back = place(1)
    for half in range(halves):
        cols = slice(half * 256, (half + 1) * 256)
        mixed = skip_ref[:, cols] * up_ref[:, cols].astype(jnp.float32)
        for read, held in ((read_r_ref[...], push_r), (-read_i_ref[...], push_i)):
            mixed = mixed + dot_nt(
                held[:, half * span : (half + 1) * span].astype(jnp.bfloat16),
                block_diagonal(read, half),
            )
        act_ref[:, cols] = dot_nn(back, jax.nn.gelu(mixed).astype(jnp.bfloat16)).astype(
            jnp.bfloat16
        )

    for copy in weights[4:]:
        copy.wait()
    pieces = out_part.shape[0]
    piece_width = out_part.shape[2]

    def piece_cols(index):
        return pl.ds(pl.multiple_of(index * piece_width, piece_width), piece_width)

    def state_piece(index, carry):
        state_part[:, piece_cols(index)] = dot_nn(
            act_ref[:, :width], w_out[:width, piece_cols(index)]
        )
        return carry

    lax.fori_loop(0, pieces, state_piece, 0)

    for pair in range(pairs):
        cols = slice(pair * LANES, (pair + 1) * LANES)
        for goal in range(2, ranks):
            if OWNERS[pair] != goal:

                @pl.when(me == goal)
                def _(pair=pair):
                    far_copy(0, pair).wait_recv()

        @pl.when(me >= 2)
        def _(pair=pair, cols=cols):
            low = run_own[:, 2 * pair * LANES : (2 * pair + 1) * LANES]
            high = run_own[:, (2 * pair + 1) * LANES : (2 * pair + 2) * LANES]
            factor = jnp.exp2(-by_head(low, high, low.shape))
            acc_own[:, cols] += factor * far_land[:, cols].astype(jnp.float32)

        act_ref[:, width + pair * LANES : width + (pair + 1) * LANES] = head_rms(
            acc_own[:, cols]
        ).astype(jnp.bfloat16)

    def part_copy(index):
        return pltpu.make_async_remote_copy(
            src_ref=out_part.at[index],
            dst_ref=out_arrived.at[index],
            send_sem=part_send.at[index],
            recv_sem=part_recv.at[index],
            **mate,
        )

    def piece_of(index, at):
        cols = piece_cols(index)
        return cols, state_part[at, cols] + dot_nn(act_ref[at, width:], w_out[width:, cols])

    def send_piece(index, carry):
        out_part[index] = piece_of(index, mate_rows)[1].astype(jnp.bfloat16)
        part_copy(index).start()
        return carry

    def own_piece(index, carry):
        cols, own = piece_of(index, own_rows)
        part_copy(index).wait_recv()
        out_ref[:, cols] = (own + out_arrived[index].astype(jnp.float32)).astype(jnp.bfloat16)
        return carry

    lax.fori_loop(0, pieces, send_piece, 0)
    lax.fori_loop(0, pieces, own_piece, 0)

    row_copy.wait_send()
    for index in range(pieces):
        part_copy(index).wait_send()
    for copy in end_copies:
        copy.wait_send()
    for origin in range(ranks):
        sent = [copy for route, copy in issued if route[1] == origin]
        if sent:

            @pl.when(me == origin)
            def _(sent=sent):
                for copy in sent:
                    copy.wait_send()

    for pair in range(pairs):
        for slot in range(2):
            if OWNERS[pair] != slot + 2:

                @pl.when(me == OWNERS[pair])
                def _(pair=pair, slot=slot):
                    far_copy(slot, pair).wait_send()


def layer(ranks, tokens, norm_gain, weights, gains, key_bias, plan):
    count, features = tokens.shape
    width = weights[0].shape[1]
    rows = key_bias.shape[0]
    states = plan[0].size
    chunks = rows // LANES
    pairs = width // LANES
    pieces = features // 512
    bias = key_bias.T
    gains = [gain[None, :] for gain in gains]
    dma = pltpu.SemaphoreType.DMA
    vmem = pl.BlockSpec(memory_space=pltpu.VMEM)
    hbm = pl.BlockSpec(memory_space=pl.ANY)
    half, full = jnp.bfloat16, jnp.float32
    return pl.pallas_call(
        functools.partial(mixer_kernel, ranks),
        out_shape=jax.ShapeDtypeStruct((count, features), jnp.bfloat16),
        in_specs=[vmem] * 2 + [hbm] * 6 + [vmem] * (3 + len(plan)),
        out_specs=vmem,
        scratch_shapes=[
            pltpu.VMEM((rows, features), half),
            pltpu.VMEM((2, states), full),
            pltpu.VMEM((rows, features), full),
            pltpu.VMEM((4, features, width), half),
            pltpu.VMEM((2 * width, features), half),
            pltpu.VMEM((rows, 2 * width), half),
            pltpu.VMEM((rows, width), half),
            pltpu.VMEM((rows, width), half),
            pltpu.VMEM((rows, width), half),
            pltpu.VMEM((rows, width), half),
            pltpu.VMEM((chunks, pairs, 2 * LANES), full),
            pltpu.VMEM((pieces, count, 512), half),
            pltpu.VMEM((pieces, count, 512), half),
            dma((6,)),
            dma((2,)),
            dma((pieces,)),
            dma((pieces,)),
            pltpu.VMEM((2, rows, width), half),
            pltpu.VMEM((2, rows, width), half),
            pltpu.VMEM((2, rows, width), half),
            pltpu.VMEM((2, chunks, pairs, 2 * LANES), full),
            pltpu.VMEM((rows, states), full),
            pltpu.VMEM((rows, states), full),
            pltpu.VMEM((rows, width), half),
            pltpu.VMEM((8, states), full),
            pltpu.VMEM((8, states), full),
            pltpu.VMEM((ranks, 2, states), full),
            pltpu.VMEM((rows, width), full),
            pltpu.VMEM((rows, 2 * width), full),
            pltpu.VMEM((2 * rows, LANES), full),
            pltpu.VMEM((2 * rows, 2 * LANES), full),
            pltpu.VMEM((2, rows, width), half),
            pltpu.VMEM((rows, width), half),
            dma((route_count(),)),
            dma((route_count(),)),
            dma((ranks,)),
            dma((ranks,)),
            dma((2, pairs)),
            dma((pairs,)),
        ],
        compiler_params=pltpu.CompilerParams(
            collective_id=0, has_side_effects=True, vmem_limit_bytes=58 * 2**20
        ),
        name="layer",
    )(tokens, norm_gain[None, :], *weights, *gains, bias, *plan)


def on_device(
    tokens,
    norm_gain,
    w_input,
    w_query,
    w_key,
    w_value,
    query_gain,
    key_gain,
    key_bias,
    eigen_real,
    eigen_imag,
    log_step,
    input_real,
    input_imag,
    read_real,
    read_imag,
    skip_gain,
    w_out_state,
    w_out_attn,
):
    ranks = lax.axis_size("sp")
    width = w_query.shape[1]
    rows = key_bias.shape[0]
    fits = (
        ranks == len(OWNERS)
        and width == ranks * LANES
        and w_input.shape[1] == width
        and width % 256 == 0
        and rows % LANES == 0
        and lax.axis_size("tp") == 2
        and tokens.shape[1] % 512 == 0
    )
    if not fits:
        return plain_device(
            tokens,
            norm_gain,
            w_input,
            w_query,
            w_key,
            w_value,
            query_gain,
            key_gain,
            key_bias,
            eigen_real,
            eigen_imag,
            log_step,
            input_real,
            input_imag,
            read_real,
            read_imag,
            skip_gain,
            w_out_state,
            w_out_attn,
        )
    ones = jnp.ones_like(eigen_real)[..., None]
    decay_r, decay_i, factor_r, factor_i = discretize(
        eigen_real, eigen_imag, log_step, ones, jnp.zeros_like(ones)
    )
    plan = (
        decay_r,
        decay_i,
        factor_r[..., 0],
        factor_i[..., 0],
        jnp.transpose(input_real, (0, 2, 1)).reshape(-1, STATE),
        jnp.transpose(input_imag, (0, 2, 1)).reshape(-1, STATE),
        read_real.reshape(-1, STATE),
        read_imag.reshape(-1, STATE),
        skip_gain[None, :],
    )
    weights = (w_input, w_query, w_key, w_value, w_out_state, w_out_attn)
    return layer(ranks, tokens, norm_gain, weights, (query_gain, key_gain), key_bias, plan)


def solution(mesh):
    placed = (
        P(("fs", "sp", "tp"), None),
        P(),
        P(None, "tp"),
        P(None, "tp"),
        P(None, "tp"),
        P(None, "tp"),
        P(),
        P(),
        P(("fs", "sp"), "tp"),
        P("tp", None),
        P("tp", None),
        P("tp"),
        P("tp", None, None),
        P("tp", None, None),
        P("tp", None, None),
        P("tp", None, None),
        P("tp"),
        P("tp", None),
        P("tp", None),
    )
    return jax.shard_map(
        on_device,
        mesh=mesh,
        in_specs=placed,
        out_specs=P(("fs", "sp", "tp"), None),
        check_vma=False,
    )
```

```python
import functools

import jax
import jax.numpy as jnp
from jax import lax
from jax.experimental import pallas as pl
from jax.experimental.pallas import tpu as pltpu
from jax.sharding import PartitionSpec as P

GROUP = 16
STATE = 64
HEAD_DIM = 64


EPSILON = 1e-06
PRECISE = lax.Precision.HIGHEST


def from_behind(block, axis, distance):
    devices = range(lax.axis_size(axis))
    route = [(i - distance, i) for i in devices if i - distance in devices]
    return lax.ppermute(block, axis, route)


def carried_in(part, axis, combine, identity):
    place = lax.axis_index(axis)
    gathered = jax.tree.map(lambda a: lax.all_gather(a, axis), part)
    state = jax.tree.map(lambda a, e: jnp.zeros_like(a) + jnp.asarray(e, a.dtype), part, identity)

    def one(lap, state):
        return combine(
            state, jax.tree.map(lambda a: lax.dynamic_index_in_dim(a, lap, 0, False), gathered)
        )

    return lax.fori_loop(0, place, one, state)


def combine_states(earlier, later):
    leading_real_factor, first_ai, first_br, first_bi = earlier
    second_ar, second_ai, second_br, second_bi = later
    prod_r = second_ar * leading_real_factor - second_ai * first_ai
    prod_i = second_ar * first_ai + second_ai * leading_real_factor
    state_r = second_ar * first_br - second_ai * first_bi + second_br
    state_i = second_ar * first_bi + second_ai * first_br + second_bi
    return (prod_r, prod_i, state_r, state_i)


def plain_discretize(eigen_real, eigen_imag, log_step, input_real, input_imag):
    step_size = jnp.exp(log_step)[:, None]
    rotation = eigen_imag * step_size
    shrink = jnp.expm1(eigen_real * step_size)
    cosine = jnp.cos(rotation)
    sine_part = jnp.sin(rotation)
    decay_r = (1.0 + shrink) * cosine
    decay_i = (1.0 + shrink) * sine_part
    minus_r = shrink * cosine - 2.0 * jnp.square(jnp.sin(0.5 * rotation))
    modulus = jnp.square(eigen_real) + jnp.square(eigen_imag)
    factor_r = (minus_r * eigen_real + decay_i * eigen_imag) / modulus
    factor_i = (decay_i * eigen_real - minus_r * eigen_imag) / modulus
    drive_r = factor_r[..., None] * input_real - factor_i[..., None] * input_imag
    drive_i = factor_r[..., None] * input_imag + factor_i[..., None] * input_real
    return (decay_r, decay_i, drive_r, drive_i)


def head_scale(flat_rows, head_gain, head_count):
    row_count = flat_rows.shape[0]
    shaped = flat_rows.astype(jnp.float32).reshape(row_count, head_count, HEAD_DIM)
    scaled = shaped * lax.rsqrt(jnp.mean(jnp.square(shaped), axis=-1, keepdims=True) + EPSILON)
    return (scaled * head_gain).astype(jnp.bfloat16)


def block_terms(queries, key_rows, value_rows, bias_rows, q_first, k_first):
    head_count = queries.shape[1]
    key_heads = key_rows.reshape(key_rows.shape[0], head_count, HEAD_DIM)
    value_heads = value_rows.reshape(value_rows.shape[0], head_count, HEAD_DIM)
    scores = jnp.einsum("qhd,khd->hqk", queries, key_heads, preferred_element_type=jnp.float32)
    scores = scores * HEAD_DIM ** (-0.5) + jnp.transpose(bias_rows.astype(jnp.float32))[:, None, :]
    query_place = q_first + lax.iota(jnp.int32, queries.shape[0])
    key_place = k_first + lax.iota(jnp.int32, key_rows.shape[0])
    causal = (key_place[None, :] < query_place[:, None])[None]
    log_keep = jnp.where(causal, jax.nn.log_sigmoid(-scores), 0.0)
    trailing_sum = lax.cumsum(log_keep, axis=2, reverse=True) - log_keep
    weights = jnp.where(causal, jnp.exp(jax.nn.log_sigmoid(scores) + trailing_sum), 0.0).astype(
        jnp.bfloat16
    )
    block_out = jnp.einsum("hqk,khd->qhd", weights, value_heads, preferred_element_type=jnp.float32)
    return (block_out.reshape(queries.shape[0], head_count * HEAD_DIM), jnp.sum(log_keep, axis=2))


def guarded_terms(queries, key_rows, value_rows, bias_rows, q_first, k_first):
    live = jnp.logical_and(k_first >= 0, k_first <= q_first)

    def compute_block():
        return block_terms(queries, key_rows, value_rows, bias_rows, q_first, k_first)

    def empty_block():
        return (
            jnp.zeros((queries.shape[0], queries.shape[1] * HEAD_DIM), jnp.float32),
            jnp.zeros((queries.shape[1], queries.shape[0]), jnp.float32),
        )

    return lax.cond(live, compute_block, empty_block)


def merge_blocks(block_parts, totals):
    blocks, row_count, row_width = block_parts.shape
    head_count = totals.shape[1]
    later_sum = jnp.flip(jnp.cumsum(jnp.flip(totals, 0), axis=0), 0) - totals
    factors = jnp.exp(jnp.transpose(later_sum, (0, 2, 1)))[..., None]

    def add_block(block_idx, accumulated):
        part = lax.dynamic_index_in_dim(block_parts, block_idx, 0, keepdims=False)
        factor = lax.dynamic_index_in_dim(factors, block_idx, 0, keepdims=False)
        return accumulated + part.reshape(row_count, head_count, HEAD_DIM) * factor

    accumulated = lax.fori_loop(
        0, blocks, add_block, jnp.zeros((row_count, head_count, HEAD_DIM), jnp.float32)
    )
    normed = accumulated * lax.rsqrt(
        jnp.mean(jnp.square(accumulated), axis=-1, keepdims=True) + EPSILON
    )
    return normed.reshape(row_count, row_width).astype(jnp.bfloat16)


def attend(queries, key_rows, value_rows, bias_rows):
    row_count = queries.shape[0]
    head_count = queries.shape[1]
    row_width = key_rows.shape[1]
    my_first = lax.axis_index("sp") * row_count
    levels = (lax.axis_size("sp") - 1).bit_length()
    slot_count = 2**levels
    own_out, own_totals = block_terms(queries, key_rows, value_rows, bias_rows, my_first, my_first)
    block_parts = lax.dynamic_update_slice_in_dim(
        jnp.zeros((slot_count, row_count, row_width), jnp.float32), own_out[None], 0, 0
    )
    totals = lax.dynamic_update_slice_in_dim(
        jnp.zeros((slot_count, head_count, row_count), jnp.float32), own_totals[None], 0, 0
    )
    held_keys = (key_rows, value_rows, bias_rows)
    for level_idx in range(levels):
        distance_base = 2**level_idx
        arrived = from_behind((held_keys[0], held_keys[1], held_keys[2]), "sp", distance_base)

        def one_block(inner_idx, current, arrived=arrived, distance_base=distance_base):
            offset = inner_idx * row_count
            distance = distance_base + inner_idx
            k_first = my_first - distance * row_count
            block_out, block_totals = guarded_terms(
                queries,
                lax.dynamic_slice_in_dim(arrived[0], offset, row_count, 0),
                lax.dynamic_slice_in_dim(arrived[1], offset, row_count, 0),
                lax.dynamic_slice_in_dim(arrived[2], offset, row_count, 0),
                my_first,
                k_first,
            )
            return (
                lax.dynamic_update_slice_in_dim(current[0], block_out[None], distance, 0),
                lax.dynamic_update_slice_in_dim(current[1], block_totals[None], distance, 0),
            )

        block_parts, totals = lax.fori_loop(0, distance_base, one_block, (block_parts, totals))
        if level_idx + 1 < levels:
            held_keys = (
                jnp.concatenate([held_keys[0], arrived[0]], axis=0),
                jnp.concatenate([held_keys[1], arrived[1]], axis=0),
                jnp.concatenate([held_keys[2], arrived[2]], axis=0),
            )
    return merge_blocks(jnp.flip(block_parts, 0), jnp.flip(totals, 0))


def state_branch(
    inputs,
    eigen_real,
    eigen_imag,
    log_step,
    input_real,
    input_imag,
    read_real,
    read_imag,
    skip_gain,
):
    decay_r, decay_i, drive_r, drive_i = plain_discretize(
        eigen_real, eigen_imag, log_step, input_real, input_imag
    )
    row_count = inputs.shape[0]
    groups = eigen_real.shape[0]
    inputs_wide = inputs.astype(jnp.float32)
    grouped = inputs_wide.reshape(row_count, groups, GROUP)
    push_r = jnp.einsum("lgh,gph->lgp", grouped, drive_r, precision=PRECISE).reshape(
        row_count, groups * STATE
    )
    push_i = jnp.einsum("lgh,gph->lgp", grouped, drive_i, precision=PRECISE).reshape(
        row_count, groups * STATE
    )
    steps_r = jnp.broadcast_to(decay_r.reshape(1, groups * STATE), push_r.shape)
    steps_i = jnp.broadcast_to(decay_i.reshape(1, groups * STATE), push_i.shape)
    running = lax.associative_scan(combine_states, (steps_r, steps_i, push_r, push_i), axis=0)
    block_ends = (
        running[0][row_count - 1],
        running[1][row_count - 1],
        running[2][row_count - 1],
        running[3][row_count - 1],
    )
    identity = (
        jnp.ones((groups * STATE,), jnp.float32),
        jnp.zeros((groups * STATE,), jnp.float32),
        jnp.zeros((groups * STATE,), jnp.float32),
        jnp.zeros((groups * STATE,), jnp.float32),
    )
    before = carried_in(block_ends, "sp", combine_states, identity)
    state_r = running[2] + running[0] * before[2][None, :] - running[1] * before[3][None, :]
    state_i = running[3] + running[0] * before[3][None, :] + running[1] * before[2][None, :]
    readout = jnp.einsum(
        "lgp,ghp->lgh", state_r.reshape(row_count, groups, STATE), read_real, precision=PRECISE
    )
    readout = readout - jnp.einsum(
        "lgp,ghp->lgh", state_i.reshape(row_count, groups, STATE), read_imag, precision=PRECISE
    )
    mixed = readout.reshape(row_count, groups * GROUP) + skip_gain * inputs_wide
    return jax.nn.gelu(mixed).astype(jnp.bfloat16)


def plain_device(
    tokens,
    norm_gain,
    w_input,
    w_query,
    w_key,
    w_value,
    query_gain,
    key_gain,
    key_bias,
    eigen_real,
    eigen_imag,
    log_step,
    input_real,
    input_imag,
    read_real,
    read_imag,
    skip_gain,
    w_out_state,
    w_out_attn,
):
    token_rows = tokens.astype(jnp.float32)
    scale_rows = lax.rsqrt(jnp.mean(jnp.square(token_rows), axis=-1, keepdims=True) + EPSILON)
    normed = (token_rows * scale_rows * norm_gain).astype(jnp.bfloat16)
    w_joined = jnp.concatenate([w_input, w_query, w_key, w_value], axis=1)
    projected = jnp.dot(
        lax.all_gather(normed, "tp", axis=0, tiled=True),
        w_joined,
        preferred_element_type=jnp.float32,
    ).astype(jnp.bfloat16)
    state_width = w_input.shape[1]
    attn_width = w_query.shape[1]
    head_count = attn_width // HEAD_DIM
    inputs = projected[:, :state_width]
    query_rows = projected[:, state_width : state_width + attn_width]
    key_rows = projected[:, state_width + attn_width : state_width + 2 * attn_width]
    value_rows = projected[:, state_width + 2 * attn_width :]
    queries = head_scale(query_rows, query_gain, head_count)
    key_normed = head_scale(key_rows, key_gain, head_count).reshape(key_rows.shape[0], attn_width)
    attn_out = attend(queries, key_normed, value_rows, key_bias)
    state_out = state_branch(
        inputs,
        eigen_real,
        eigen_imag,
        log_step,
        input_real,
        input_imag,
        read_real,
        read_imag,
        skip_gain,
    )
    summed_part = jnp.dot(state_out, w_out_state, preferred_element_type=jnp.float32)
    return lax.psum_scatter(
        (summed_part + jnp.dot(attn_out, w_out_attn, preferred_element_type=jnp.float32)).astype(
            jnp.bfloat16
        ),
        "tp",
        scatter_dimension=0,
        tiled=True,
    )


LANES = 128
NT = (((1,), (1,)), ((), ()))


def dot_nt(a, b):
    return lax.dot_general(a, b, NT, preferred_element_type=jnp.float32)


def dot_nn(a, b):
    return jnp.dot(a, b, preferred_element_type=jnp.float32)


def by_head(low, high, shape):
    return jnp.where(lax.broadcasted_iota(jnp.int32, shape, 1) < HEAD_DIM, low, high)


def head_rms(rows):
    square = rows * rows
    low = jnp.sum(by_head(square, 0.0, rows.shape), axis=-1, keepdims=True)
    high = jnp.sum(by_head(0.0, square, rows.shape), axis=-1, keepdims=True)
    mean = by_head(low, high, rows.shape) * (1.0 / HEAD_DIM)
    return rows * lax.rsqrt(mean + EPSILON)


def complex_power(real, imag, exponent):
    out_r, out_i = None, None
    while exponent:
        if exponent & 1:
            if out_r is None:
                out_r, out_i = real, imag
            else:
                out_r, out_i = out_r * real - out_i * imag, out_r * imag + out_i * real
        exponent >>= 1
        if exponent:
            real, imag = real * real - imag * imag, 2.0 * real * imag
    return out_r, out_i


LOG2E = 1.4426950408889634
OWNERS = (0, 1, 1, 2)
KINDS = "kvq"


def pairs_of(owner):
    return [pair for pair, rank in reversed(list(enumerate(OWNERS))) if rank == owner]


LATE = 2


def routes(kind, origin, late=0):
    every = list(reversed(range(len(OWNERS))))
    if late == 1:
        plan = {0: [(1, 0, pairs_of(1))]}
    elif late == 2:
        plan = {0: [(1, 0, pairs_of(0))], 2: [(3, 0, every[LATE:])]}
    elif kind == "q":
        plan = {
            2: [(0, 0, pairs_of(0)), (1, 0, pairs_of(1))],
            3: [(0, 1, pairs_of(0)), (1, 1, pairs_of(1)), (2, 1, pairs_of(2))],
        }
    else:
        plan = {
            0: [(1, 0, pairs_of(2))],
            1: [(2, 1, pairs_of(2)), (0, 1, pairs_of(0))],
            2: [(3, 0, every[:LATE])],
        }
    return [(goal, slot, pair) for goal, slot, held in plan.get(origin, []) for pair in held]


BIASES = ((0, 1, 0), (1, 0, 1), (0, 2, 0), (1, 2, 1), (2, 3, 0))


def small_expm1(value):
    series = jnp.ones_like(value)
    for order in range(9, 1, -1):
        series = 1.0 + value * series * (1.0 / order)
    return jnp.where(value > -0.5, value * series, jnp.exp(value) - 1.0)


def discretize(eigen_real, eigen_imag, log_step):
    groups = eigen_real.shape[0]
    diagonal = lax.broadcasted_iota(jnp.int32, (groups, groups), 0) == lax.broadcasted_iota(
        jnp.int32, (groups, groups), 1
    )
    step_row = jnp.broadcast_to(jnp.exp(log_step), (groups, groups))
    step_size = jnp.sum(jnp.where(diagonal, step_row, 0.0), axis=1, keepdims=True)
    rotation = eigen_imag * step_size
    shrink = small_expm1(eigen_real * step_size)
    cosine = jnp.cos(rotation)
    sine_part = jnp.sin(rotation)
    half_sine = jnp.sin(0.5 * rotation)
    decay_r = (1.0 + shrink) * cosine
    decay_i = (1.0 + shrink) * sine_part
    minus_r = shrink * cosine - 2.0 * half_sine * half_sine
    modulus = eigen_real * eigen_real + eigen_imag * eigen_imag
    factor_r = (minus_r * eigen_real + decay_i * eigen_imag) / modulus
    factor_i = (decay_i * eigen_real - minus_r * eigen_imag) / modulus
    return decay_r, decay_i, factor_r, factor_i


def mixer_kernel(
    ranks,
    tokens_ref,
    norm_gain_ref,
    w_input_ref,
    w_query_ref,
    w_key_ref,
    w_value_ref,
    w_state_ref,
    w_attn_ref,
    q_gain_ref,
    k_gain_ref,
    bias_ref,
    eigen_r_ref,
    eigen_i_ref,
    log_step_ref,
    input_r_ref,
    input_i_ref,
    read_r_ref,
    read_i_ref,
    skip_ref,
    out_ref,
    plan_ref,
    normed,
    decay_ref,
    state_part,
    w_held,
    w_out,
    act_ref,
    u_ref,
    v_ref,
    q_norm,
    k_norm,
    bias_stage,
    out_part,
    out_arrived,
    w_sem,
    row_sem,
    part_send,
    part_recv,
    q_far,
    k_far,
    v_far,
    bias_far,
    push_r,
    push_i,
    up_ref,
    seg_r,
    seg_i,
    ends_land,
    acc_own,
    run_own,
    acc_far,
    run_far,
    far_stage,
    far_land,
    route_send,
    route_recv,
    bias_send,
    bias_recv,
    end_send,
    end_recv,
    back_send,
    back_recv,
):
    rows, width = u_ref.shape
    states = decay_ref.shape[1]
    chunks = rows // LANES
    pairs = width // LANES
    seg_len = rows // 8
    own_count, features = tokens_ref.shape
    core = lax.axis_index("tp")
    own_rows = pl.ds(pl.multiple_of(core * own_count, own_count), own_count)
    mate_rows = pl.ds(pl.multiple_of((1 - core) * own_count, own_count), own_count)
    mate = {"device_id": {"tp": 1 - core}, "device_id_type": pl.DeviceIdType.MESH}
    halves = width // 256
    span = states // halves
    me = lax.axis_index("sp")
    others = range(1, ranks)

    def at_rank(step):
        return lax.rem(me + step, ranks)

    barrier = pltpu.get_barrier_semaphore()
    for step in others:
        pl.semaphore_signal(
            barrier, inc=1, device_id={"sp": at_rank(step)}, device_id_type=pl.DeviceIdType.MESH
        )

    pl.semaphore_signal(barrier, inc=1, **mate)
    weights = []
    for slot, ref in enumerate((w_key_ref, w_value_ref, w_query_ref, w_input_ref)):
        weights.append(pltpu.make_async_copy(ref, w_held.at[slot], w_sem.at[slot]))
    for slot, ref in enumerate((w_state_ref, w_attn_ref)):
        target = w_out.at[slot * width : (slot + 1) * width, :]
        weights.append(pltpu.make_async_copy(ref, target, w_sem.at[4 + slot]))
    for low, order in ((True, (0, 1, 2)), (False, (2, 0, 1))):

        @pl.when((me < 2) if low else (me >= 2))
        def _(order=order):
            for slot in order:
                weights[slot].start()


    token_rows = tokens_ref[...].astype(jnp.float32)
    mean = jnp.sum(token_rows * token_rows, axis=-1, keepdims=True) * (1.0 / features)
    scaled = token_rows * lax.rsqrt(mean + EPSILON) * norm_gain_ref[...]
    normed[own_rows, :] = scaled.astype(jnp.bfloat16)
    bias = bias_ref[...].astype(jnp.float32) * LOG2E
    for chunk in range(chunks):
        for head in range(2 * pairs):
            lanes = slice((head % 2) * LANES, (head % 2 + 1) * LANES)
            bias_stage[chunk, head // 2 : head // 2 + 1, lanes] = bias[
                head : head + 1, chunk * LANES : (chunk + 1) * LANES
            ]
    q_gain, k_gain = (
        jnp.concatenate([ref[...], ref[...]], axis=1) for ref in (q_gain_ref, k_gain_ref)
    )
    q_gain = q_gain * (LOG2E * HEAD_DIM**-0.5)
    groups = eigen_r_ref.shape[0]
    plan = discretize(eigen_r_ref[...], eigen_i_ref[...], log_step_ref[...])
    for row, value in enumerate(plan):
        plan_ref[row] = value
    for row in range(2):
        decay_ref[row : row + 1, :] = jnp.concatenate(
            [plan_ref[row, group : group + 1, :] for group in range(groups)], axis=1
        )

    sources = (k_norm, v_ref, q_norm)
    targets = (k_far, v_far, q_far)
    sent = {rank: [] for rank in range(ranks)}

    def piece_copy(kind, goal, slot, pair, part, relay=False):
        at = (own_rows, mate_rows)[part]
        cols = pair_cols(pair)
        target = targets[kind].at[slot, at, cols]
        return pltpu.make_async_remote_copy(
            src_ref=target if relay else sources[kind].at[at, cols],
            dst_ref=target,
            send_sem=route_send.at[kind, int(relay), pair, part],
            recv_sem=route_recv.at[kind, slot, pair, part],
            device_id={"sp": goal},
            device_id_type=pl.DeviceIdType.MESH,
        )

    def bias_copy(index):
        _, goal, slot = BIASES[index]
        return pltpu.make_async_remote_copy(
            src_ref=bias_stage,
            dst_ref=bias_far.at[slot],
            send_sem=bias_send.at[index],
            recv_sem=bias_recv.at[slot],
            device_id={"sp": goal},
            device_id_type=pl.DeviceIdType.MESH,
        )

    def send_entries(entries, origin):
        sent[origin] += entries

        @pl.when(me == origin)
        def _():
            for entry in entries:
                piece_copy(*entry).start()

    def send_pieces(kind, part, ranks_of):
        for origin in ranks_of:
            chosen = routes(KINDS[kind], origin)
            if chosen:
                send_entries([(kind, *route, part) for route in chosen], origin)

    def send_late(ranks_of, late):
        for origin in ranks_of:
            chosen = routes("k", origin, late)
            if chosen:
                send_entries(
                    [
                        (kind, *route, part)
                        for route in chosen
                        for kind in range(2)
                        for part in range(2)
                    ],
                    origin,
                )

    def arrive(kind, slot, pair):
        for part in range(2):
            piece_copy(kind, 0, slot, pair, part).wait_recv()

    def pair_cols(pair):
        if isinstance(pair, int):
            return slice(pair * LANES, (pair + 1) * LANES)
        return pl.ds(pl.multiple_of(pair * LANES, LANES), LANES)

    pl.semaphore_wait(barrier, ranks)
    row_copy = pltpu.make_async_remote_copy(
        src_ref=normed.at[own_rows, :],
        dst_ref=normed.at[own_rows, :],
        send_sem=row_sem.at[0],
        recv_sem=row_sem.at[1],
        **mate,
    )
    row_copy.start()
    for copy in weights[3:]:
        copy.start()
    for index, (origin, _, _) in enumerate(BIASES):
        sent[origin].append((index,))

        @pl.when(me == origin)
        def _(index=index):
            bias_copy(index).start()


    def project(slot, at):
        flat = dot_nn(normed[at, :], w_held[slot]).astype(jnp.bfloat16)
        if slot == 1:
            v_ref[at, :] = flat
        elif slot == 3:
            u_ref[at, :] = flat
        else:
            gain, target = (k_gain, k_norm) if slot == 0 else (q_gain, q_norm)
            for tile in range(width // LANES):
                cols = slice(tile * LANES, (tile + 1) * LANES)
                part = head_rms(flat[:, cols].astype(jnp.float32)) * gain
                target[at, cols] = part.astype(jnp.bfloat16)

    low_order, high_order = (0, 1, 2), (2, 0, 1)

    def project_part(part, at):
        for ranks_of, order in (((0, 1), low_order), ((2, 3), high_order)):
            @pl.when((me < 2) if order is low_order else (me >= 2))
            def _(ranks_of=ranks_of, order=order):
                for kind in order:
                    if part == 0:
                        weights[kind].wait()
                    project(kind, at)
                    send_pieces(kind, part, ranks_of)
                if part == 1 and 0 in ranks_of:
                    send_late((0,), 1)

    project_part(0, own_rows)
    row_copy.wait_recv()
    project_part(1, mate_rows)
    whole = slice(0, rows)
    tail = lax.broadcasted_iota(jnp.int32, (2 * LANES, 2 * LANES), 0)
    col = lax.broadcasted_iota(jnp.int32, (2 * LANES, 2 * LANES), 1)
    tail = jnp.where(
        jnp.logical_and(tail >= col, tail // LANES == col // LANES), 1.0, 0.0
    ).astype(jnp.bfloat16)
    lane = lax.broadcasted_iota(jnp.int32, (1, LANES), 1)
    low_mask = jnp.where(lane < HEAD_DIM, 1.0, 0.0).astype(jnp.bfloat16)
    high_mask = jnp.where(lane < HEAD_DIM, 0.0, 1.0).astype(jnp.bfloat16)

    def both_heads(block):
        return jnp.concatenate([block * low_mask, block * high_mask], axis=0)

    def attend(streams):
        scores, softs, masks, sums = [], [], [], []
        for queries, blocks, _, diagonal in streams:
            for keys, _, bias_row, first in blocks:
                z = dot_nt(queries[first:], both_heads(keys)) + bias_row
                scores.append(z)
                if diagonal:
                    masks.append(
                        (lax.broadcasted_iota(jnp.int32, z.shape, 1) & (LANES - 1))
                        < lax.broadcasted_iota(jnp.int32, z.shape, 0)
                    )
                else:
                    masks.append(None)
        for z, mask in zip(scores, masks):
            soft = jnp.log(1.0 + jnp.exp2(z)) * LOG2E
            if mask is not None:
                soft = jnp.where(mask, soft, 0.0)
            softs.append(soft.astype(jnp.bfloat16))
        for soft in softs:
            sums.append(dot_nn(soft, tail))
        results = []
        at = 0
        for queries, blocks, running, diagonal in streams:
            probs, values, out = [], [], None
            for _, block, _, first in blocks:
                z, mask, inner = scores[at], masks[at], sums[at]
                at += 1
                count = z.shape[0]
                if running.shape[0] < count:
                    fresh = jnp.zeros((count - running.shape[0], 2 * LANES), jnp.float32)
                    running = jnp.concatenate([fresh, running], axis=0)
                weight = jnp.exp2(z - (inner + running))
                if mask is not None:
                    weight = jnp.where(mask, weight, 0.0)
                totals = [
                    jnp.broadcast_to(inner[:, head * LANES : head * LANES + 1], (count, LANES))
                    for head in range(2)
                ]
                running = running + jnp.concatenate(totals, axis=1)
                if diagonal:
                    part = dot_nn(weight.astype(jnp.bfloat16), both_heads(block))
                    if out is not None:
                        fresh = part.shape[0] - out.shape[0]
                        part = jnp.concatenate([part[:fresh], part[fresh:] + out], axis=0)
                    out = part
                else:
                    probs.append(weight.astype(jnp.bfloat16))
                    values.append(both_heads(block))
            if not diagonal:
                out = dot_nn(jnp.concatenate(probs, axis=1), jnp.concatenate(values, axis=0))
            results.append((out, running))
        return results

    def run_cols(pair):
        return pl.ds(pl.multiple_of(pair * 2 * LANES, 2 * LANES), 2 * LANES)

    group = 2

    def own_group(step, carry):
        held = [step * group + index for index in range(group)]
        streams = []
        for pair in held:
            cols = pair_cols(pair)
            blocks = [
                (
                    k_norm[chunk * LANES : (chunk + 1) * LANES, cols],
                    v_ref[chunk * LANES : (chunk + 1) * LANES, cols],
                    bias_stage[chunk, pl.ds(pair, 1), :],
                    chunk * LANES,
                )
                for chunk in reversed(range(chunks))
            ]
            none = jnp.zeros((LANES, 2 * LANES), jnp.float32)
            streams.append((q_norm[:, cols], blocks, none, True))
        for pair, (out, running) in zip(held, attend(streams)):
            acc_own[:, pair_cols(pair)] = out
            run_own[:, run_cols(pair)] = running
        return carry

    def near_group(step, carry):
        held = [pairs - 1 - step * group - index for index in range(group)]
        for pair in held:
            for pending in (me == 3, jnp.logical_and(me == 1, pair < len(pairs_of(0)))):

                @pl.when(pending)
                def _(pair=pair):
                    for kind in range(2):
                        arrive(kind, 0, pair)

        streams = []
        for pair in held:
            cols = pair_cols(pair)
            blocks = [
                (
                    k_far[0, chunk * LANES : (chunk + 1) * LANES, cols],
                    v_far[0, chunk * LANES : (chunk + 1) * LANES, cols],
                    bias_far[0, chunk, pl.ds(pair, 1), :],
                    0,
                )
                for chunk in reversed(range(chunks))
            ]
            streams.append((q_norm[:, cols], blocks, run_own[:, run_cols(pair)], False))
        for pair, (out, running) in zip(held, attend(streams)):
            acc_own[:, pair_cols(pair)] += out
            run_own[:, run_cols(pair)] = running
        return carry

    def far_copy(slot, pair):
        return pltpu.make_async_remote_copy(
            src_ref=far_stage.at[slot, :, pair_cols(pair)],
            dst_ref=far_land.at[:, pair_cols(pair)],
            send_sem=back_send.at[slot, pair],
            recv_sem=back_recv.at[pair],
            device_id={"sp": slot + 2},
            device_id_type=pl.DeviceIdType.MESH,
        )

    def far_pair(step, carry):
        pair = last_pair - 1 - step
        cols = pair_cols(pair)
        for owner, due in enumerate(
            (
                ((2, 0), (2, 1), (0, 1), (1, 1)),
                ((2, 0), (2, 1), (0, 0), (1, 0)),
                ((2, 1), (0, 1), (1, 1), (0, 0), (1, 0)),
            )
        ):

            @pl.when(me == owner)
            def _(due=due):
                for kind, slot in due:
                    arrive(kind, slot, pair)

        queries = q_far[:, :, cols].reshape(2 * rows, LANES)
        acc_far[...] = jnp.zeros_like(acc_far)
        run_far[...] = jnp.zeros_like(run_far)

        def key_block(step, inner):
            slot = 1 - step
            blocks = [
                (
                    k_far[slot, chunk * LANES : (chunk + 1) * LANES, cols],
                    v_far[slot, chunk * LANES : (chunk + 1) * LANES, cols],
                    bias_far[slot, chunk, pl.ds(pair, 1), :],
                    0,
                )
                for chunk in reversed(range(chunks))
            ]
            ((out, running),) = attend([(queries, blocks, run_far[...], False)])
            acc_far[...] += out
            run_far[...] = running
            return inner

        lax.fori_loop(0, 2, key_block, 0)
        for slot in range(2):
            part = acc_far[slot * rows : (slot + 1) * rows, :].astype(jnp.bfloat16)

            @pl.when(me == slot + 2)
            def _(part=part):
                far_land[:, cols] = part

            @pl.when(me != slot + 2)
            def _(part=part, slot=slot):
                far_stage[slot, :, cols] = part
                far_copy(slot, pair).start()

        return carry

    far_count, last_pair = jnp.int32(0), jnp.int32(0)
    for owner in range(3):
        if pairs_of(owner):
            far_count = jnp.where(me == owner, len(pairs_of(owner)), far_count)
            last_pair = jnp.where(me == owner, pairs_of(owner)[0] + 1, last_pair)

    lax.fori_loop(0, pairs // group, own_group, 0)
    for owner, (slot, held) in enumerate(
        (
            (0, ((k_norm, k_far), (v_ref, v_far), (bias_stage, bias_far))),
            (1, ((k_norm, k_far), (v_ref, v_far), (bias_stage, bias_far))),
            (0, ((q_norm, q_far),)),
        )
    ):

        @pl.when(me == owner)
        def _(slot=slot, held=held):
            for source, target in held:
                target[slot] = source[...]

    for pair in pairs_of(2):
        relayed = [(kind, 2, 0, pair, part, True) for part in range(2) for kind in range(2)]
        sent[1] += relayed

        @pl.when(me == 1)
        def _(relayed=relayed, pair=pair):
            for kind in range(2):
                arrive(kind, 0, pair)
            for entry in relayed:
                piece_copy(*entry).start()

    for goal in range(ranks):
        for index, (_, target, _) in enumerate(BIASES):
            if target == goal:

                @pl.when(me == goal)
                def _(index=index):
                    bias_copy(index).wait_recv()

    far_first = 0
    weights[3].wait()
    project(3, whole)

    def place(axis):
        index = lax.broadcasted_iota(jnp.int32, (rows, rows), axis)
        other = lax.broadcasted_iota(jnp.int32, (rows, rows), 1 - axis)
        return jnp.where(other == (index & 7) * seg_len + (index >> 3), 1.0, 0.0).astype(
            jnp.bfloat16
        )

    up_ref[...] = dot_nn(place(0), u_ref[...]).astype(jnp.bfloat16)

    spread_state = lax.broadcasted_iota(jnp.int32, (STATE, span), 0) == (
        lax.broadcasted_iota(jnp.int32, (STATE, span), 1) & (STATE - 1)
    )
    spread_state = jnp.where(spread_state, 1.0, 0.0).astype(jnp.bfloat16)

    def by_channel(row):
        wide = jnp.broadcast_to(plan_ref[row][:, None, :], (groups, GROUP, STATE))
        return wide.reshape(groups * GROUP, STATE)

    factor_r = by_channel(2)
    factor_i = by_channel(3)
    drive_r = factor_r * input_r_ref[...] - factor_i * input_i_ref[...]
    drive_i = factor_r * input_i_ref[...] + factor_i * input_r_ref[...]

    def block_diagonal(values, half):
        row_group = lax.broadcasted_iota(jnp.int32, (256, span), 0) // GROUP
        col_group = lax.broadcasted_iota(jnp.int32, (256, span), 1) // STATE
        wide = dot_nn(
            values[half * 256 : (half + 1) * 256, :].astype(jnp.bfloat16), spread_state
        )
        return jnp.where(row_group == col_group, wide, 0.0).astype(jnp.bfloat16)

    for half in range(halves):
        cols = slice(half * span, (half + 1) * span)
        part = up_ref[:, half * 256 : (half + 1) * 256]
        push_r[:, cols] = dot_nn(part, block_diagonal(drive_r, half))
        push_i[:, cols] = dot_nn(part, block_diagonal(drive_i, half))

    block = 512

    def scan(keep_states):
        for first in range(0, states, block):
            cols = slice(first, first + block)
            step_r = jnp.broadcast_to(decay_ref[0:1, cols], (8, block))
            step_i = jnp.broadcast_to(decay_ref[1:2, cols], (8, block))

            def one(index, state, cols=cols, step_r=step_r, step_i=step_i):
                state_r, state_i = state
                at = pl.ds(pl.multiple_of(index * 8, 8), 8)
                next_r = step_r * state_r - step_i * state_i + push_r[at, cols]
                next_i = step_r * state_i + step_i * state_r + push_i[at, cols]
                if keep_states:
                    push_r[at, cols] = next_r
                    push_i[at, cols] = next_i
                return (next_r, next_i)

            if keep_states:
                start = (seg_r[:, cols], seg_i[:, cols])
            else:
                start = (jnp.zeros((8, block), jnp.float32),) * 2
            state_r, state_i = lax.fori_loop(0, seg_len, one, start, unroll=4)
            if not keep_states:
                seg_r[:, cols] = state_r
                seg_i[:, cols] = state_i

    scan(False)
    seg_step_r, seg_step_i = complex_power(decay_ref[0:1, :], decay_ref[1:2, :], seg_len)
    end_r = jnp.zeros((1, states), jnp.float32)
    end_i = jnp.zeros((1, states), jnp.float32)
    for seg in range(8):
        end_r, end_i = (
            seg_step_r * end_r - seg_step_i * end_i + seg_r[seg : seg + 1, :],
            seg_step_r * end_i + seg_step_i * end_r + seg_i[seg : seg + 1, :],
        )
    ends_land[me, 0:1, :] = end_r
    ends_land[me, 1:2, :] = end_i
    end_copies = []
    for step in others:
        copy = pltpu.make_async_remote_copy(
            src_ref=ends_land.at[me],
            dst_ref=ends_land.at[me],
            send_sem=end_send.at[step],
            recv_sem=end_recv.at[step],
            device_id={"sp": at_rank(step)},
            device_id_type=pl.DeviceIdType.MESH,
        )
        copy.start()
        end_copies.append(copy)

    send_late((0, 2), 2)
    lax.fori_loop(far_first, far_count, far_pair, 0)

    for copy in end_copies:
        copy.wait_recv()
    block_r, block_i = complex_power(decay_ref[0:1, :], decay_ref[1:2, :], rows)
    carry_r = jnp.zeros((1, states), jnp.float32)
    carry_i = jnp.zeros((1, states), jnp.float32)
    for rank in range(ranks - 1):
        next_r = block_r * carry_r - block_i * carry_i + ends_land[rank, 0:1, :]
        next_i = block_r * carry_i + block_i * carry_r + ends_land[rank, 1:2, :]
        carry_r = jnp.where(rank < me, next_r, carry_r)
        carry_i = jnp.where(rank < me, next_i, carry_i)
    for seg in range(8):
        own_r = seg_r[seg : seg + 1, :]
        own_i = seg_i[seg : seg + 1, :]
        seg_r[seg : seg + 1, :] = carry_r
        seg_i[seg : seg + 1, :] = carry_i
        carry_r, carry_i = (
            seg_step_r * carry_r - seg_step_i * carry_i + own_r,
            seg_step_r * carry_i + seg_step_i * carry_r + own_i,
        )
    scan(True)

    back = place(1)
    for half in range(halves):
        cols = slice(half * 256, (half + 1) * 256)
        mixed = skip_ref[:, cols] * up_ref[:, cols].astype(jnp.float32)
        for read, held in ((read_r_ref[...], push_r), (-read_i_ref[...], push_i)):
            mixed = mixed + dot_nt(
                held[:, half * span : (half + 1) * span].astype(jnp.bfloat16),
                block_diagonal(read, half),
            )
        act_ref[:, cols] = dot_nn(back, jax.nn.gelu(mixed).astype(jnp.bfloat16)).astype(
            jnp.bfloat16
        )

    for copy in weights[4:]:
        copy.wait()
    pieces = out_part.shape[0]
    piece_width = out_part.shape[2]

    def piece_cols(index):
        return pl.ds(pl.multiple_of(index * piece_width, piece_width), piece_width)

    def state_piece(index, carry):
        state_part[:, piece_cols(index)] = dot_nn(
            act_ref[:, :width], w_out[:width, piece_cols(index)]
        )
        return carry

    lax.fori_loop(0, pieces, state_piece, 0)

    @pl.when(lax.rem(me, 2) == 1)
    def _():
        lax.fori_loop(0, pairs // group, near_group, 0)


    for pair in range(pairs):
        cols = slice(pair * LANES, (pair + 1) * LANES)
        for goal in range(2, ranks):
            if OWNERS[pair] != goal:

                @pl.when(me == goal)
                def _(pair=pair):
                    far_copy(0, pair).wait_recv()

        @pl.when(me >= 2)
        def _(pair=pair, cols=cols):
            low = run_own[:, 2 * pair * LANES : (2 * pair + 1) * LANES]
            high = run_own[:, (2 * pair + 1) * LANES : (2 * pair + 2) * LANES]
            factor = jnp.exp2(-by_head(low, high, low.shape))
            acc_own[:, cols] += factor * far_land[:, cols].astype(jnp.float32)

        act_ref[:, width + pair * LANES : width + (pair + 1) * LANES] = head_rms(
            acc_own[:, cols]
        ).astype(jnp.bfloat16)

    def part_copy(index):
        return pltpu.make_async_remote_copy(
            src_ref=out_part.at[index],
            dst_ref=out_arrived.at[index],
            send_sem=part_send.at[index],
            recv_sem=part_recv.at[index],
            **mate,
        )

    def piece_of(index, at):
        cols = piece_cols(index)
        return cols, state_part[at, cols] + dot_nn(act_ref[at, width:], w_out[width:, cols])

    def send_piece(index, carry):
        out_part[index] = piece_of(index, mate_rows)[1].astype(jnp.bfloat16)
        part_copy(index).start()
        return carry

    def own_piece(index, carry):
        cols, own = piece_of(index, own_rows)
        part_copy(index).wait_recv()
        out_ref[:, cols] = (own + out_arrived[index].astype(jnp.float32)).astype(jnp.bfloat16)
        return carry

    lax.fori_loop(0, pieces, send_piece, 0)
    lax.fori_loop(0, pieces, own_piece, 0)

    row_copy.wait_send()
    for index in range(pieces):
        part_copy(index).wait_send()
    for copy in end_copies:
        copy.wait_send()
    for origin in range(ranks):

        @pl.when(me == origin)
        def _(entries=sent[origin]):
            for entry in entries:
                (piece_copy if len(entry) > 1 else bias_copy)(*entry).wait_send()

    for pair in range(pairs):
        for slot in range(2):
            if OWNERS[pair] != slot + 2:

                @pl.when(me == OWNERS[pair])
                def _(pair=pair, slot=slot):
                    far_copy(slot, pair).wait_send()


def layer(ranks, tokens, norm_gain, weights, gains, key_bias, plan):
    count, features = tokens.shape
    width = weights[0].shape[1]
    rows = key_bias.shape[0]
    states = plan[0].size
    chunks = rows // LANES
    pairs = width // LANES
    pieces = features // 512
    bias = key_bias.T
    gains = [gain[None, :] for gain in gains]
    dma = pltpu.SemaphoreType.DMA
    vmem = pl.BlockSpec(memory_space=pltpu.VMEM)
    hbm = pl.BlockSpec(memory_space=pl.ANY)
    half, full = jnp.bfloat16, jnp.float32
    return pl.pallas_call(
        functools.partial(mixer_kernel, ranks),
        out_shape=jax.ShapeDtypeStruct((count, features), jnp.bfloat16),
        in_specs=[vmem] * 2 + [hbm] * 6 + [vmem] * (3 + len(plan)),
        out_specs=vmem,
        scratch_shapes=[
            pltpu.VMEM((4, *plan[0].shape), full),
            pltpu.VMEM((rows, features), half),
            pltpu.VMEM((2, states), full),
            pltpu.VMEM((rows, features), full),
            pltpu.VMEM((4, features, width), half),
            pltpu.VMEM((2 * width, features), half),
            pltpu.VMEM((rows, 2 * width), half),
            pltpu.VMEM((rows, width), half),
            pltpu.VMEM((rows, width), half),
            pltpu.VMEM((rows, width), half),
            pltpu.VMEM((rows, width), half),
            pltpu.VMEM((chunks, pairs, 2 * LANES), full),
            pltpu.VMEM((pieces, count, 512), half),
            pltpu.VMEM((pieces, count, 512), half),
            dma((6,)),
            dma((2,)),
            dma((pieces,)),
            dma((pieces,)),
            pltpu.VMEM((2, rows, width), half),
            pltpu.VMEM((2, rows, width), half),
            pltpu.VMEM((2, rows, width), half),
            pltpu.VMEM((2, chunks, pairs, 2 * LANES), full),
            pltpu.VMEM((rows, states), full),
            pltpu.VMEM((rows, states), full),
            pltpu.VMEM((rows, width), half),
            pltpu.VMEM((8, states), full),
            pltpu.VMEM((8, states), full),
            pltpu.VMEM((ranks, 2, states), full),
            pltpu.VMEM((rows, width), full),
            pltpu.VMEM((rows, 2 * width), full),
            pltpu.VMEM((2 * rows, LANES), full),
            pltpu.VMEM((2 * rows, 2 * LANES), full),
            pltpu.VMEM((2, rows, width), half),
            pltpu.VMEM((rows, width), half),
            dma((3, 2, pairs, 2)),
            dma((3, 2, pairs, 2)),
            dma((len(BIASES),)),
            dma((2,)),
            dma((ranks,)),
            dma((ranks,)),
            dma((2, pairs)),
            dma((pairs,)),
        ],
        compiler_params=pltpu.CompilerParams(
            collective_id=0, has_side_effects=True, vmem_limit_bytes=58 * 2**20
        ),
        name="layer",
    )(tokens, norm_gain[None, :], *weights, *gains, bias, *plan)


def on_device(
    tokens,
    norm_gain,
    w_input,
    w_query,
    w_key,
    w_value,
    query_gain,
    key_gain,
    key_bias,
    eigen_real,
    eigen_imag,
    log_step,
    input_real,
    input_imag,
    read_real,
    read_imag,
    skip_gain,
    w_out_state,
    w_out_attn,
):
    ranks = lax.axis_size("sp")
    width = w_query.shape[1]
    rows = key_bias.shape[0]
    fits = (
        ranks == len(OWNERS)
        and width == ranks * LANES
        and w_input.shape[1] == width
        and width % 256 == 0
        and rows % LANES == 0
        and lax.axis_size("tp") == 2
        and tokens.shape[1] % 512 == 0
    )
    if not fits:
        return plain_device(
            tokens,
            norm_gain,
            w_input,
            w_query,
            w_key,
            w_value,
            query_gain,
            key_gain,
            key_bias,
            eigen_real,
            eigen_imag,
            log_step,
            input_real,
            input_imag,
            read_real,
            read_imag,
            skip_gain,
            w_out_state,
            w_out_attn,
        )
    plan = (
        eigen_real,
        eigen_imag,
        log_step[None, :],
        jnp.transpose(input_real, (0, 2, 1)).reshape(-1, STATE),
        jnp.transpose(input_imag, (0, 2, 1)).reshape(-1, STATE),
        read_real.reshape(-1, STATE),
        read_imag.reshape(-1, STATE),
        skip_gain[None, :],
    )
    weights = (w_input, w_query, w_key, w_value, w_out_state, w_out_attn)
    return layer(ranks, tokens, norm_gain, weights, (query_gain, key_gain), key_bias, plan)


def solution(mesh):
    placed = (
        P(("fs", "sp", "tp"), None),
        P(),
        P(None, "tp"),
        P(None, "tp"),
        P(None, "tp"),
        P(None, "tp"),
        P(),
        P(),
        P(("fs", "sp"), "tp"),
        P("tp", None),
        P("tp", None),
        P("tp"),
        P("tp", None, None),
        P("tp", None, None),
        P("tp", None, None),
        P("tp", None, None),
        P("tp"),
        P("tp", None),
        P("tp", None),
    )
    return jax.shard_map(
        on_device,
        mesh=mesh,
        in_specs=placed,
        out_specs=P(("fs", "sp", "tp"), None),
        check_vma=False,
    )
```

```python
import functools

import jax
import jax.numpy as jnp
from jax import lax
from jax.experimental import pallas as pl
from jax.experimental.pallas import tpu as pltpu
from jax.sharding import PartitionSpec as P

GROUP = 16
STATE = 64
HEAD_DIM = 64


EPSILON = 1e-06
PRECISE = lax.Precision.HIGHEST


def from_behind(block, axis, distance):
    devices = range(lax.axis_size(axis))
    route = [(i - distance, i) for i in devices if i - distance in devices]
    return lax.ppermute(block, axis, route)


def carried_in(part, axis, combine, identity):
    place = lax.axis_index(axis)
    gathered = jax.tree.map(lambda a: lax.all_gather(a, axis), part)
    state = jax.tree.map(lambda a, e: jnp.zeros_like(a) + jnp.asarray(e, a.dtype), part, identity)

    def one(lap, state):
        return combine(
            state, jax.tree.map(lambda a: lax.dynamic_index_in_dim(a, lap, 0, False), gathered)
        )

    return lax.fori_loop(0, place, one, state)


def combine_states(earlier, later):
    leading_real_factor, first_ai, first_br, first_bi = earlier
    second_ar, second_ai, second_br, second_bi = later
    prod_r = second_ar * leading_real_factor - second_ai * first_ai
    prod_i = second_ar * first_ai + second_ai * leading_real_factor
    state_r = second_ar * first_br - second_ai * first_bi + second_br
    state_i = second_ar * first_bi + second_ai * first_br + second_bi
    return (prod_r, prod_i, state_r, state_i)


def plain_discretize(eigen_real, eigen_imag, log_step, input_real, input_imag):
    step_size = jnp.exp(log_step)[:, None]
    rotation = eigen_imag * step_size
    shrink = jnp.expm1(eigen_real * step_size)
    cosine = jnp.cos(rotation)
    sine_part = jnp.sin(rotation)
    decay_r = (1.0 + shrink) * cosine
    decay_i = (1.0 + shrink) * sine_part
    minus_r = shrink * cosine - 2.0 * jnp.square(jnp.sin(0.5 * rotation))
    modulus = jnp.square(eigen_real) + jnp.square(eigen_imag)
    factor_r = (minus_r * eigen_real + decay_i * eigen_imag) / modulus
    factor_i = (decay_i * eigen_real - minus_r * eigen_imag) / modulus
    drive_r = factor_r[..., None] * input_real - factor_i[..., None] * input_imag
    drive_i = factor_r[..., None] * input_imag + factor_i[..., None] * input_real
    return (decay_r, decay_i, drive_r, drive_i)


def head_scale(flat_rows, head_gain, head_count):
    row_count = flat_rows.shape[0]
    shaped = flat_rows.astype(jnp.float32).reshape(row_count, head_count, HEAD_DIM)
    scaled = shaped * lax.rsqrt(jnp.mean(jnp.square(shaped), axis=-1, keepdims=True) + EPSILON)
    return (scaled * head_gain).astype(jnp.bfloat16)


def block_terms(queries, key_rows, value_rows, bias_rows, q_first, k_first):
    head_count = queries.shape[1]
    key_heads = key_rows.reshape(key_rows.shape[0], head_count, HEAD_DIM)
    value_heads = value_rows.reshape(value_rows.shape[0], head_count, HEAD_DIM)
    scores = jnp.einsum("qhd,khd->hqk", queries, key_heads, preferred_element_type=jnp.float32)
    scores = scores * HEAD_DIM ** (-0.5) + jnp.transpose(bias_rows.astype(jnp.float32))[:, None, :]
    query_place = q_first + lax.iota(jnp.int32, queries.shape[0])
    key_place = k_first + lax.iota(jnp.int32, key_rows.shape[0])
    causal = (key_place[None, :] < query_place[:, None])[None]
    log_keep = jnp.where(causal, jax.nn.log_sigmoid(-scores), 0.0)
    trailing_sum = lax.cumsum(log_keep, axis=2, reverse=True) - log_keep
    weights = jnp.where(causal, jnp.exp(jax.nn.log_sigmoid(scores) + trailing_sum), 0.0).astype(
        jnp.bfloat16
    )
    block_out = jnp.einsum("hqk,khd->qhd", weights, value_heads, preferred_element_type=jnp.float32)
    return (block_out.reshape(queries.shape[0], head_count * HEAD_DIM), jnp.sum(log_keep, axis=2))


def guarded_terms(queries, key_rows, value_rows, bias_rows, q_first, k_first):
    live = jnp.logical_and(k_first >= 0, k_first <= q_first)

    def compute_block():
        return block_terms(queries, key_rows, value_rows, bias_rows, q_first, k_first)

    def empty_block():
        return (
            jnp.zeros((queries.shape[0], queries.shape[1] * HEAD_DIM), jnp.float32),
            jnp.zeros((queries.shape[1], queries.shape[0]), jnp.float32),
        )

    return lax.cond(live, compute_block, empty_block)


def merge_blocks(block_parts, totals):
    blocks, row_count, row_width = block_parts.shape
    head_count = totals.shape[1]
    later_sum = jnp.flip(jnp.cumsum(jnp.flip(totals, 0), axis=0), 0) - totals
    factors = jnp.exp(jnp.transpose(later_sum, (0, 2, 1)))[..., None]

    def add_block(block_idx, accumulated):
        part = lax.dynamic_index_in_dim(block_parts, block_idx, 0, keepdims=False)
        factor = lax.dynamic_index_in_dim(factors, block_idx, 0, keepdims=False)
        return accumulated + part.reshape(row_count, head_count, HEAD_DIM) * factor

    accumulated = lax.fori_loop(
        0, blocks, add_block, jnp.zeros((row_count, head_count, HEAD_DIM), jnp.float32)
    )
    normed = accumulated * lax.rsqrt(
        jnp.mean(jnp.square(accumulated), axis=-1, keepdims=True) + EPSILON
    )
    return normed.reshape(row_count, row_width).astype(jnp.bfloat16)


def attend(queries, key_rows, value_rows, bias_rows):
    row_count = queries.shape[0]
    head_count = queries.shape[1]
    row_width = key_rows.shape[1]
    my_first = lax.axis_index("sp") * row_count
    levels = (lax.axis_size("sp") - 1).bit_length()
    slot_count = 2**levels
    own_out, own_totals = block_terms(queries, key_rows, value_rows, bias_rows, my_first, my_first)
    block_parts = lax.dynamic_update_slice_in_dim(
        jnp.zeros((slot_count, row_count, row_width), jnp.float32), own_out[None], 0, 0
    )
    totals = lax.dynamic_update_slice_in_dim(
        jnp.zeros((slot_count, head_count, row_count), jnp.float32), own_totals[None], 0, 0
    )
    held_keys = (key_rows, value_rows, bias_rows)
    for level_idx in range(levels):
        distance_base = 2**level_idx
        arrived = from_behind((held_keys[0], held_keys[1], held_keys[2]), "sp", distance_base)

        def one_block(inner_idx, current, arrived=arrived, distance_base=distance_base):
            offset = inner_idx * row_count
            distance = distance_base + inner_idx
            k_first = my_first - distance * row_count
            block_out, block_totals = guarded_terms(
                queries,
                lax.dynamic_slice_in_dim(arrived[0], offset, row_count, 0),
                lax.dynamic_slice_in_dim(arrived[1], offset, row_count, 0),
                lax.dynamic_slice_in_dim(arrived[2], offset, row_count, 0),
                my_first,
                k_first,
            )
            return (
                lax.dynamic_update_slice_in_dim(current[0], block_out[None], distance, 0),
                lax.dynamic_update_slice_in_dim(current[1], block_totals[None], distance, 0),
            )

        block_parts, totals = lax.fori_loop(0, distance_base, one_block, (block_parts, totals))
        if level_idx + 1 < levels:
            held_keys = (
                jnp.concatenate([held_keys[0], arrived[0]], axis=0),
                jnp.concatenate([held_keys[1], arrived[1]], axis=0),
                jnp.concatenate([held_keys[2], arrived[2]], axis=0),
            )
    return merge_blocks(jnp.flip(block_parts, 0), jnp.flip(totals, 0))


def state_branch(
    inputs,
    eigen_real,
    eigen_imag,
    log_step,
    input_real,
    input_imag,
    read_real,
    read_imag,
    skip_gain,
):
    decay_r, decay_i, drive_r, drive_i = plain_discretize(
        eigen_real, eigen_imag, log_step, input_real, input_imag
    )
    row_count = inputs.shape[0]
    groups = eigen_real.shape[0]
    inputs_wide = inputs.astype(jnp.float32)
    grouped = inputs_wide.reshape(row_count, groups, GROUP)
    push_r = jnp.einsum("lgh,gph->lgp", grouped, drive_r, precision=PRECISE).reshape(
        row_count, groups * STATE
    )
    push_i = jnp.einsum("lgh,gph->lgp", grouped, drive_i, precision=PRECISE).reshape(
        row_count, groups * STATE
    )
    steps_r = jnp.broadcast_to(decay_r.reshape(1, groups * STATE), push_r.shape)
    steps_i = jnp.broadcast_to(decay_i.reshape(1, groups * STATE), push_i.shape)
    running = lax.associative_scan(combine_states, (steps_r, steps_i, push_r, push_i), axis=0)
    block_ends = (
        running[0][row_count - 1],
        running[1][row_count - 1],
        running[2][row_count - 1],
        running[3][row_count - 1],
    )
    identity = (
        jnp.ones((groups * STATE,), jnp.float32),
        jnp.zeros((groups * STATE,), jnp.float32),
        jnp.zeros((groups * STATE,), jnp.float32),
        jnp.zeros((groups * STATE,), jnp.float32),
    )
    before = carried_in(block_ends, "sp", combine_states, identity)
    state_r = running[2] + running[0] * before[2][None, :] - running[1] * before[3][None, :]
    state_i = running[3] + running[0] * before[3][None, :] + running[1] * before[2][None, :]
    readout = jnp.einsum(
        "lgp,ghp->lgh", state_r.reshape(row_count, groups, STATE), read_real, precision=PRECISE
    )
    readout = readout - jnp.einsum(
        "lgp,ghp->lgh", state_i.reshape(row_count, groups, STATE), read_imag, precision=PRECISE
    )
    mixed = readout.reshape(row_count, groups * GROUP) + skip_gain * inputs_wide
    return jax.nn.gelu(mixed).astype(jnp.bfloat16)


def plain_device(
    tokens,
    norm_gain,
    w_input,
    w_query,
    w_key,
    w_value,
    query_gain,
    key_gain,
    key_bias,
    eigen_real,
    eigen_imag,
    log_step,
    input_real,
    input_imag,
    read_real,
    read_imag,
    skip_gain,
    w_out_state,
    w_out_attn,
):
    token_rows = tokens.astype(jnp.float32)
    scale_rows = lax.rsqrt(jnp.mean(jnp.square(token_rows), axis=-1, keepdims=True) + EPSILON)
    normed = (token_rows * scale_rows * norm_gain).astype(jnp.bfloat16)
    w_joined = jnp.concatenate([w_input, w_query, w_key, w_value], axis=1)
    projected = jnp.dot(
        lax.all_gather(normed, "tp", axis=0, tiled=True),
        w_joined,
        preferred_element_type=jnp.float32,
    ).astype(jnp.bfloat16)
    state_width = w_input.shape[1]
    attn_width = w_query.shape[1]
    head_count = attn_width // HEAD_DIM
    inputs = projected[:, :state_width]
    query_rows = projected[:, state_width : state_width + attn_width]
    key_rows = projected[:, state_width + attn_width : state_width + 2 * attn_width]
    value_rows = projected[:, state_width + 2 * attn_width :]
    queries = head_scale(query_rows, query_gain, head_count)
    key_normed = head_scale(key_rows, key_gain, head_count).reshape(key_rows.shape[0], attn_width)
    attn_out = attend(queries, key_normed, value_rows, key_bias)
    state_out = state_branch(
        inputs,
        eigen_real,
        eigen_imag,
        log_step,
        input_real,
        input_imag,
        read_real,
        read_imag,
        skip_gain,
    )
    summed_part = jnp.dot(state_out, w_out_state, preferred_element_type=jnp.float32)
    return lax.psum_scatter(
        (summed_part + jnp.dot(attn_out, w_out_attn, preferred_element_type=jnp.float32)).astype(
            jnp.bfloat16
        ),
        "tp",
        scatter_dimension=0,
        tiled=True,
    )


LANES = 128
NT = (((1,), (1,)), ((), ()))


def dot_nt(a, b):
    return lax.dot_general(a, b, NT, preferred_element_type=jnp.float32)


def dot_nn(a, b):
    return jnp.dot(a, b, preferred_element_type=jnp.float32)


def by_head(low, high, shape):
    return jnp.where(lax.broadcasted_iota(jnp.int32, shape, 1) < HEAD_DIM, low, high)


def head_rms(rows):
    square = rows * rows
    low = jnp.sum(by_head(square, 0.0, rows.shape), axis=-1, keepdims=True)
    high = jnp.sum(by_head(0.0, square, rows.shape), axis=-1, keepdims=True)
    mean = by_head(low, high, rows.shape) * (1.0 / HEAD_DIM)
    return rows * lax.rsqrt(mean + EPSILON)


def complex_power(real, imag, exponent):
    out_r, out_i = None, None
    while exponent:
        if exponent & 1:
            if out_r is None:
                out_r, out_i = real, imag
            else:
                out_r, out_i = out_r * real - out_i * imag, out_r * imag + out_i * real
        exponent >>= 1
        if exponent:
            real, imag = real * real - imag * imag, 2.0 * real * imag
    return out_r, out_i


LOG2E = 1.4426950408889634
OWNERS = (0, 1, 1, 2)
KINDS = "kvq"


def pairs_of(owner):
    return [pair for pair, rank in reversed(list(enumerate(OWNERS))) if rank == owner]


LAST_MERGED = min(pairs_of(1) or [0])
MERGED = [pair for pair in range(len(OWNERS)) if pair != LAST_MERGED] + [LAST_MERGED]


def routes(kind, origin, late=0):
    every = list(reversed(range(len(OWNERS))))
    if late == 1:
        plan = {0: [(1, 0, pairs_of(1))]}
    elif late == 2:
        plan = {0: [(1, 0, pairs_of(0))]}
    elif kind == "q":
        plan = {
            2: [(0, 0, pairs_of(0)), (1, 0, pairs_of(1))],
            3: [(0, 1, pairs_of(0)), (1, 1, pairs_of(1)), (2, 1, pairs_of(2))],
        }
    else:
        plan = {
            0: [(1, 0, pairs_of(2))],
            1: [(2, 1, pairs_of(2)), (0, 1, pairs_of(0))],
            2: [(3, 0, [pair for pair in every if OWNERS[pair] != 2])],
        }
    return [(goal, slot, pair) for goal, slot, held in plan.get(origin, []) for pair in held]


BIASES = ((0, 1, 0), (1, 0, 1), (0, 2, 0), (1, 2, 1), (2, 3, 0))


def small_expm1(value):
    series = jnp.ones_like(value)
    for order in range(9, 1, -1):
        series = 1.0 + value * series * (1.0 / order)
    return jnp.where(value > -0.5, value * series, jnp.exp(value) - 1.0)


def discretize(eigen_real, eigen_imag, log_step):
    groups = eigen_real.shape[0]
    diagonal = lax.broadcasted_iota(jnp.int32, (groups, groups), 0) == lax.broadcasted_iota(
        jnp.int32, (groups, groups), 1
    )
    step_row = jnp.broadcast_to(jnp.exp(log_step), (groups, groups))
    step_size = jnp.sum(jnp.where(diagonal, step_row, 0.0), axis=1, keepdims=True)
    rotation = eigen_imag * step_size
    shrink = small_expm1(eigen_real * step_size)
    cosine = jnp.cos(rotation)
    sine_part = jnp.sin(rotation)
    half_sine = jnp.sin(0.5 * rotation)
    decay_r = (1.0 + shrink) * cosine
    decay_i = (1.0 + shrink) * sine_part
    minus_r = shrink * cosine - 2.0 * half_sine * half_sine
    modulus = eigen_real * eigen_real + eigen_imag * eigen_imag
    factor_r = (minus_r * eigen_real + decay_i * eigen_imag) / modulus
    factor_i = (decay_i * eigen_real - minus_r * eigen_imag) / modulus
    return decay_r, decay_i, factor_r, factor_i


def mixer_kernel(
    ranks,
    tokens_ref,
    norm_gain_ref,
    w_input_ref,
    w_query_ref,
    w_key_ref,
    w_value_ref,
    w_state_ref,
    w_attn_ref,
    q_gain_ref,
    k_gain_ref,
    bias_ref,
    eigen_r_ref,
    eigen_i_ref,
    log_step_ref,
    input_r_ref,
    input_i_ref,
    read_r_ref,
    read_i_ref,
    skip_ref,
    out_ref,
    plan_ref,
    normed,
    decay_ref,
    state_part,
    w_held,
    w_out,
    act_ref,
    u_ref,
    v_ref,
    q_norm,
    k_norm,
    bias_stage,
    out_part,
    out_arrived,
    w_sem,
    row_sem,
    part_send,
    part_recv,
    q_far,
    k_far,
    v_far,
    bias_far,
    push_r,
    push_i,
    up_ref,
    seg_r,
    seg_i,
    ends_land,
    acc_own,
    run_own,
    acc_far,
    run_far,
    far_stage,
    far_land,
    route_send,
    route_recv,
    bias_send,
    bias_recv,
    end_send,
    end_recv,
    back_send,
    back_recv,
):
    rows, width = u_ref.shape
    states = decay_ref.shape[1]
    chunks = rows // LANES
    pairs = width // LANES
    seg_len = rows // 8
    own_count, features = tokens_ref.shape
    core = lax.axis_index("tp")
    own_rows = pl.ds(pl.multiple_of(core * own_count, own_count), own_count)
    mate_rows = pl.ds(pl.multiple_of((1 - core) * own_count, own_count), own_count)
    mate = {"device_id": {"tp": 1 - core}, "device_id_type": pl.DeviceIdType.MESH}
    halves = width // 256
    span = states // halves
    me = lax.axis_index("sp")
    others = range(1, ranks)

    def at_rank(step):
        return lax.rem(me + step, ranks)

    barrier = pltpu.get_barrier_semaphore()
    for step in others:
        pl.semaphore_signal(
            barrier, inc=1, device_id={"sp": at_rank(step)}, device_id_type=pl.DeviceIdType.MESH
        )

    pl.semaphore_signal(barrier, inc=1, **mate)
    weights = []
    for slot, ref in enumerate((w_key_ref, w_value_ref, w_query_ref, w_input_ref)):
        weights.append(pltpu.make_async_copy(ref, w_held.at[slot], w_sem.at[slot]))
    weights.append(pltpu.make_async_copy(w_state_ref, w_out.at[:width, :], w_sem.at[4]))
    for place_of, pair in enumerate(MERGED):
        first = width + place_of * LANES
        weights.append(
            pltpu.make_async_copy(
                w_attn_ref.at[pair * LANES : (pair + 1) * LANES, :],
                w_out.at[first : first + LANES, :],
                w_sem.at[5 + place_of],
            )
        )
    for low, order in ((True, (0, 1, 2)), (False, (2, 0, 1))):

        @pl.when((me < 2) if low else (me >= 2))
        def _(order=order):
            for slot in order:
                weights[slot].start()


    token_rows = tokens_ref[...].astype(jnp.float32)
    mean = jnp.sum(token_rows * token_rows, axis=-1, keepdims=True) * (1.0 / features)
    scaled = token_rows * lax.rsqrt(mean + EPSILON) * norm_gain_ref[...]
    normed[own_rows, :] = scaled.astype(jnp.bfloat16)
    bias = bias_ref[...].astype(jnp.float32) * LOG2E
    for chunk in range(chunks):
        for head in range(2 * pairs):
            lanes = slice((head % 2) * LANES, (head % 2 + 1) * LANES)
            bias_stage[chunk, head // 2 : head // 2 + 1, lanes] = bias[
                head : head + 1, chunk * LANES : (chunk + 1) * LANES
            ]
    q_gain, k_gain = (
        jnp.concatenate([ref[...], ref[...]], axis=1) for ref in (q_gain_ref, k_gain_ref)
    )
    q_gain = q_gain * (LOG2E * HEAD_DIM**-0.5)
    groups = eigen_r_ref.shape[0]
    plan = discretize(eigen_r_ref[...], eigen_i_ref[...], log_step_ref[...])
    for row, value in enumerate(plan):
        plan_ref[row] = value
    for row in range(2):
        decay_ref[row : row + 1, :] = jnp.concatenate(
            [plan_ref[row, group : group + 1, :] for group in range(groups)], axis=1
        )

    sources = (k_norm, v_ref, q_norm)
    targets = (k_far, v_far, q_far)
    sent = {rank: [] for rank in range(ranks)}

    def piece_copy(kind, goal, slot, pair, part, relay=False):
        at = (own_rows, mate_rows)[part]
        cols = pair_cols(pair)
        target = targets[kind].at[slot, at, cols]
        return pltpu.make_async_remote_copy(
            src_ref=target if relay else sources[kind].at[at, cols],
            dst_ref=target,
            send_sem=route_send.at[kind, int(relay), pair, part],
            recv_sem=route_recv.at[kind, slot, pair, part],
            device_id={"sp": goal},
            device_id_type=pl.DeviceIdType.MESH,
        )

    def bias_copy(index):
        _, goal, slot = BIASES[index]
        return pltpu.make_async_remote_copy(
            src_ref=bias_stage,
            dst_ref=bias_far.at[slot],
            send_sem=bias_send.at[index],
            recv_sem=bias_recv.at[slot],
            device_id={"sp": goal},
            device_id_type=pl.DeviceIdType.MESH,
        )

    def send_entries(entries, origin):
        sent[origin] += entries

        @pl.when(me == origin)
        def _():
            for entry in entries:
                piece_copy(*entry).start()

    def send_pieces(kind, part, ranks_of):
        for origin in ranks_of:
            chosen = routes(KINDS[kind], origin)
            leading = [route for route in chosen if route[0] == 0 or kind < 2]
            entries = [(kind, *route, part) for route in leading]
            if part == 1:
                entries += [
                    (kind, *route, at) for route in chosen if route not in leading for at in range(2)
                ]
            if entries:
                send_entries(entries, origin)

    def send_late(ranks_of, late):
        for origin in ranks_of:
            chosen = routes("k", origin, late)
            if chosen:
                send_entries(
                    [
                        (kind, *route, part)
                        for route in chosen
                        for kind in range(2)
                        for part in range(2)
                    ],
                    origin,
                )

    def arrive(kind, slot, pair):
        for part in range(2):
            piece_copy(kind, 0, slot, pair, part).wait_recv()

    def pair_cols(pair):
        if isinstance(pair, int):
            return slice(pair * LANES, (pair + 1) * LANES)
        return pl.ds(pl.multiple_of(pair * LANES, LANES), LANES)

    pl.semaphore_wait(barrier, ranks)
    row_copy = pltpu.make_async_remote_copy(
        src_ref=normed.at[own_rows, :],
        dst_ref=normed.at[own_rows, :],
        send_sem=row_sem.at[0],
        recv_sem=row_sem.at[1],
        **mate,
    )
    row_copy.start()
    for copy in weights[3:]:
        copy.start()
    for index, (origin, _, _) in enumerate(BIASES):
        sent[origin].append((index,))

        @pl.when(me == origin)
        def _(index=index):
            bias_copy(index).start()


    def project(slot, at):
        flat = dot_nn(normed[at, :], w_held[slot]).astype(jnp.bfloat16)
        if slot == 1:
            v_ref[at, :] = flat
        elif slot == 3:
            u_ref[at, :] = flat
        else:
            gain, target = (k_gain, k_norm) if slot == 0 else (q_gain, q_norm)
            for tile in range(width // LANES):
                cols = slice(tile * LANES, (tile + 1) * LANES)
                part = head_rms(flat[:, cols].astype(jnp.float32)) * gain
                target[at, cols] = part.astype(jnp.bfloat16)

    low_order, high_order = (0, 1, 2), (2, 0, 1)

    def project_part(part, at):
        for ranks_of, order in (((0, 1), low_order), ((2, 3), high_order)):
            @pl.when((me < 2) if order is low_order else (me >= 2))
            def _(ranks_of=ranks_of, order=order):
                for kind in order:
                    if part == 0:
                        weights[kind].wait()
                    project(kind, at)
                    send_pieces(kind, part, ranks_of)
                if part == 1 and 0 in ranks_of:
                    send_late((0,), 1)

    project_part(0, own_rows)
    row_copy.wait_recv()
    project_part(1, mate_rows)
    whole = slice(0, rows)
    tail = lax.broadcasted_iota(jnp.int32, (2 * LANES, 2 * LANES), 0)
    col = lax.broadcasted_iota(jnp.int32, (2 * LANES, 2 * LANES), 1)
    tail = jnp.where(
        jnp.logical_and(tail >= col, tail // LANES == col // LANES), 1.0, 0.0
    ).astype(jnp.bfloat16)
    lane = lax.broadcasted_iota(jnp.int32, (1, LANES), 1)
    low_mask = jnp.where(lane < HEAD_DIM, 1.0, 0.0).astype(jnp.bfloat16)
    high_mask = jnp.where(lane < HEAD_DIM, 0.0, 1.0).astype(jnp.bfloat16)

    def both_heads(block):
        return jnp.concatenate([block * low_mask, block * high_mask], axis=0)

    def attend(streams):
        scores, softs, masks, sums = [], [], [], []
        for queries, blocks, _, diagonal in streams:
            for keys, _, bias_row, first in blocks:
                z = dot_nt(queries[first:], both_heads(keys)) + bias_row
                scores.append(z)
                if diagonal:
                    masks.append(
                        (lax.broadcasted_iota(jnp.int32, z.shape, 1) & (LANES - 1))
                        < lax.broadcasted_iota(jnp.int32, z.shape, 0)
                    )
                else:
                    masks.append(None)
        for z, mask in zip(scores, masks):
            soft = jnp.log(1.0 + jnp.exp2(z)) * LOG2E
            if mask is not None:
                soft = jnp.where(mask, soft, 0.0)
            softs.append(soft.astype(jnp.bfloat16))
        for soft in softs:
            sums.append(dot_nn(soft, tail))
        results = []
        at = 0
        for queries, blocks, running, diagonal in streams:
            probs, values, out = [], [], None
            for _, block, _, first in blocks:
                z, mask, inner = scores[at], masks[at], sums[at]
                at += 1
                count = z.shape[0]
                if running.shape[0] < count:
                    fresh = jnp.zeros((count - running.shape[0], 2 * LANES), jnp.float32)
                    running = jnp.concatenate([fresh, running], axis=0)
                weight = jnp.exp2(z - (inner + running))
                if mask is not None:
                    weight = jnp.where(mask, weight, 0.0)
                totals = [
                    jnp.broadcast_to(inner[:, head * LANES : head * LANES + 1], (count, LANES))
                    for head in range(2)
                ]
                running = running + jnp.concatenate(totals, axis=1)
                if diagonal:
                    part = dot_nn(weight.astype(jnp.bfloat16), both_heads(block))
                    if out is not None:
                        fresh = part.shape[0] - out.shape[0]
                        part = jnp.concatenate([part[:fresh], part[fresh:] + out], axis=0)
                    out = part
                else:
                    probs.append(weight.astype(jnp.bfloat16))
                    values.append(both_heads(block))
            if not diagonal:
                out = dot_nn(jnp.concatenate(probs, axis=1), jnp.concatenate(values, axis=0))
            results.append((out, running))
        return results

    def run_cols(pair):
        return pl.ds(pl.multiple_of(pair * 2 * LANES, 2 * LANES), 2 * LANES)

    group = 2

    def own_group(step, carry):
        held = [step * group + index for index in range(group)]
        streams = []
        for pair in held:
            cols = pair_cols(pair)
            blocks = [
                (
                    k_norm[chunk * LANES : (chunk + 1) * LANES, cols],
                    v_ref[chunk * LANES : (chunk + 1) * LANES, cols],
                    bias_stage[chunk, pl.ds(pair, 1), :],
                    chunk * LANES,
                )
                for chunk in reversed(range(chunks))
            ]
            none = jnp.zeros((LANES, 2 * LANES), jnp.float32)
            streams.append((q_norm[:, cols], blocks, none, True))
        for pair, (out, running) in zip(held, attend(streams)):
            acc_own[:, pair_cols(pair)] = out
            run_own[:, run_cols(pair)] = running
        return carry

    def near_group(step, carry):
        held = [pairs - 1 - step]
        for pair in held:
            for pending in (me == 3, jnp.logical_and(me == 1, pair < len(pairs_of(0)))):

                @pl.when(pending)
                def _(pair=pair):
                    for kind in range(2):
                        arrive(kind, 0, pair)

        streams = []
        for pair in held:
            cols = pair_cols(pair)
            blocks = [
                (
                    k_far[0, chunk * LANES : (chunk + 1) * LANES, cols],
                    v_far[0, chunk * LANES : (chunk + 1) * LANES, cols],
                    bias_far[0, chunk, pl.ds(pair, 1), :],
                    0,
                )
                for chunk in reversed(range(chunks))
            ]
            streams.append((q_norm[:, cols], blocks, run_own[:, run_cols(pair)], False))
        for pair, (out, running) in zip(held, attend(streams)):
            acc_own[:, pair_cols(pair)] += out
            run_own[:, run_cols(pair)] = running
        return carry

    def far_copy(slot, pair):
        return pltpu.make_async_remote_copy(
            src_ref=far_stage.at[slot, :, pair_cols(pair)],
            dst_ref=far_land.at[:, pair_cols(pair)],
            send_sem=back_send.at[slot, pair],
            recv_sem=back_recv.at[pair],
            device_id={"sp": slot + 2},
            device_id_type=pl.DeviceIdType.MESH,
        )

    def far_pair(step, carry):
        pair = last_pair - 1 - step
        cols = pair_cols(pair)
        acc_far[...] = jnp.zeros_like(acc_far)
        run_far[...] = jnp.zeros_like(run_far)

        @pl.when(me == 2)
        def _():
            arrive(2, 1, pair)
            blocks = [
                (
                    k_norm[chunk * LANES : (chunk + 1) * LANES, cols],
                    v_ref[chunk * LANES : (chunk + 1) * LANES, cols],
                    bias_stage[chunk, pl.ds(pair, 1), :],
                    0,
                )
                for chunk in reversed(range(chunks))
            ]
            ((out, running),) = attend([(q_far[1, :, cols], blocks, run_far[rows:, :], False)])
            acc_far[rows:, :] = out
            run_far[rows:, :] = running

        for owner, due in enumerate(
            (
                ((2, 0), (2, 1), (0, 1), (1, 1)),
                ((2, 0), (2, 1), (0, 0), (1, 0)),
                ((0, 1), (1, 1), (0, 0), (1, 0)),
            )
        ):

            @pl.when(me == owner)
            def _(due=due):
                for kind, slot in due:
                    arrive(kind, slot, pair)

        queries = q_far[:, :, cols].reshape(2 * rows, LANES)
        def key_block(step, inner):
            slot = 1 - step
            blocks = [
                (
                    k_far[slot, chunk * LANES : (chunk + 1) * LANES, cols],
                    v_far[slot, chunk * LANES : (chunk + 1) * LANES, cols],
                    bias_far[slot, chunk, pl.ds(pair, 1), :],
                    0,
                )
                for chunk in reversed(range(chunks))
            ]
            ((out, running),) = attend([(queries, blocks, run_far[...], False)])
            acc_far[...] += out
            run_far[...] = running
            return inner

        lax.fori_loop(0, 2, key_block, 0)
        for slot in range(2):
            part = acc_far[slot * rows : (slot + 1) * rows, :].astype(jnp.bfloat16)

            @pl.when(me == slot + 2)
            def _(part=part):
                far_land[:, cols] = part

            @pl.when(me != slot + 2)
            def _(part=part, slot=slot):
                far_stage[slot, :, cols] = part
                far_copy(slot, pair).start()

        return carry

    far_count, last_pair = jnp.int32(0), jnp.int32(0)
    for owner in range(3):
        if pairs_of(owner):
            far_count = jnp.where(me == owner, len(pairs_of(owner)), far_count)
            last_pair = jnp.where(me == owner, pairs_of(owner)[0] + 1, last_pair)

    lax.fori_loop(0, pairs // group, own_group, 0)
    for owner, (slot, held) in enumerate(
        (
            (0, ((k_norm, k_far), (v_ref, v_far), (bias_stage, bias_far))),
            (1, ((k_norm, k_far), (v_ref, v_far), (bias_stage, bias_far))),
            (0, ((q_norm, q_far),)),
        )
    ):

        @pl.when(me == owner)
        def _(slot=slot, held=held):
            for source, target in held:
                target[slot] = source[...]

    for goal in range(ranks):
        for index, (_, target, _) in enumerate(BIASES):
            if target == goal:

                @pl.when(me == goal)
                def _(index=index):
                    bias_copy(index).wait_recv()

    weights[3].wait()
    project(3, whole)

    def place(axis):
        index = lax.broadcasted_iota(jnp.int32, (rows, rows), axis)
        other = lax.broadcasted_iota(jnp.int32, (rows, rows), 1 - axis)
        return jnp.where(other == (index & 7) * seg_len + (index >> 3), 1.0, 0.0).astype(
            jnp.bfloat16
        )

    up_ref[...] = dot_nn(place(0), u_ref[...]).astype(jnp.bfloat16)

    for pair in pairs_of(2):
        relayed = [(kind, 2, 0, pair, part, True) for part in range(2) for kind in range(2)]
        sent[1] += relayed

        @pl.when(me == 1)
        def _(relayed=relayed, pair=pair):
            for kind in range(2):
                arrive(kind, 0, pair)
            for entry in relayed:
                piece_copy(*entry).start()


    spread_state = lax.broadcasted_iota(jnp.int32, (STATE, span), 0) == (
        lax.broadcasted_iota(jnp.int32, (STATE, span), 1) & (STATE - 1)
    )
    spread_state = jnp.where(spread_state, 1.0, 0.0).astype(jnp.bfloat16)

    def by_channel(row):
        wide = jnp.broadcast_to(plan_ref[row][:, None, :], (groups, GROUP, STATE))
        return wide.reshape(groups * GROUP, STATE)

    factor_r = by_channel(2)
    factor_i = by_channel(3)
    drive_r = factor_r * input_r_ref[...] - factor_i * input_i_ref[...]
    drive_i = factor_r * input_i_ref[...] + factor_i * input_r_ref[...]

    def block_diagonal(values, half):
        row_group = lax.broadcasted_iota(jnp.int32, (256, span), 0) // GROUP
        col_group = lax.broadcasted_iota(jnp.int32, (256, span), 1) // STATE
        wide = dot_nn(
            values[half * 256 : (half + 1) * 256, :].astype(jnp.bfloat16), spread_state
        )
        return jnp.where(row_group == col_group, wide, 0.0).astype(jnp.bfloat16)

    for half in range(halves):
        cols = slice(half * span, (half + 1) * span)
        part = up_ref[:, half * 256 : (half + 1) * 256]
        push_r[:, cols] = dot_nn(part, block_diagonal(drive_r, half))
        push_i[:, cols] = dot_nn(part, block_diagonal(drive_i, half))

    block = 512

    def scan(keep_states):
        for first in range(0, states, block):
            cols = slice(first, first + block)
            step_r = jnp.broadcast_to(decay_ref[0:1, cols], (8, block))
            step_i = jnp.broadcast_to(decay_ref[1:2, cols], (8, block))

            def one(index, state, cols=cols, step_r=step_r, step_i=step_i):
                state_r, state_i = state
                at = pl.ds(pl.multiple_of(index * 8, 8), 8)
                next_r = step_r * state_r - step_i * state_i + push_r[at, cols]
                next_i = step_r * state_i + step_i * state_r + push_i[at, cols]
                if keep_states:
                    push_r[at, cols] = next_r
                    push_i[at, cols] = next_i
                return (next_r, next_i)

            if keep_states:
                start = (seg_r[:, cols], seg_i[:, cols])
            else:
                start = (jnp.zeros((8, block), jnp.float32),) * 2
            state_r, state_i = lax.fori_loop(0, seg_len, one, start, unroll=4)
            if not keep_states:
                seg_r[:, cols] = state_r
                seg_i[:, cols] = state_i

    scan(False)
    seg_step_r, seg_step_i = complex_power(decay_ref[0:1, :], decay_ref[1:2, :], seg_len)
    end_r = jnp.zeros((1, states), jnp.float32)
    end_i = jnp.zeros((1, states), jnp.float32)
    for seg in range(8):
        end_r, end_i = (
            seg_step_r * end_r - seg_step_i * end_i + seg_r[seg : seg + 1, :],
            seg_step_r * end_i + seg_step_i * end_r + seg_i[seg : seg + 1, :],
        )
    ends_land[me, 0:1, :] = end_r
    ends_land[me, 1:2, :] = end_i
    end_copies = []
    for step in others:
        copy = pltpu.make_async_remote_copy(
            src_ref=ends_land.at[me],
            dst_ref=ends_land.at[me],
            send_sem=end_send.at[step],
            recv_sem=end_recv.at[step],
            device_id={"sp": at_rank(step)},
            device_id_type=pl.DeviceIdType.MESH,
        )
        copy.start()
        end_copies.append(copy)

    send_late((0,), 2)
    far_middle = jnp.where(me == 1, jnp.minimum(far_count, 1), far_count)
    near_first = jnp.where(me == 3, len(pairs_of(2)), 0)
    near_count = jnp.where(lax.rem(me, 2) == 1, pairs, 0)
    near_middle = jnp.where(me == 1, len(pairs_of(2)) + 1, near_count)
    near_start = jnp.where(me == 1, len(pairs_of(2)), near_count)
    lax.fori_loop(near_first, near_start, near_group, 0)
    lax.fori_loop(0, far_middle, far_pair, 0)
    lax.fori_loop(near_start, near_middle, near_group, 0)
    lax.fori_loop(far_middle, far_count, far_pair, 0)

    for copy in end_copies:
        copy.wait_recv()
    block_r, block_i = complex_power(decay_ref[0:1, :], decay_ref[1:2, :], rows)
    carry_r = jnp.zeros((1, states), jnp.float32)
    carry_i = jnp.zeros((1, states), jnp.float32)
    for rank in range(ranks - 1):
        next_r = block_r * carry_r - block_i * carry_i + ends_land[rank, 0:1, :]
        next_i = block_r * carry_i + block_i * carry_r + ends_land[rank, 1:2, :]
        carry_r = jnp.where(rank < me, next_r, carry_r)
        carry_i = jnp.where(rank < me, next_i, carry_i)
    for seg in range(8):
        own_r = seg_r[seg : seg + 1, :]
        own_i = seg_i[seg : seg + 1, :]
        seg_r[seg : seg + 1, :] = carry_r
        seg_i[seg : seg + 1, :] = carry_i
        carry_r, carry_i = (
            seg_step_r * carry_r - seg_step_i * carry_i + own_r,
            seg_step_r * carry_i + seg_step_i * carry_r + own_i,
        )
    scan(True)

    back = place(1)
    for half in range(halves):
        cols = slice(half * 256, (half + 1) * 256)
        mixed = skip_ref[:, cols] * up_ref[:, cols].astype(jnp.float32)
        for read, held in ((read_r_ref[...], push_r), (-read_i_ref[...], push_i)):
            mixed = mixed + dot_nt(
                held[:, half * span : (half + 1) * span].astype(jnp.bfloat16),
                block_diagonal(read, half),
            )
        act_ref[:, cols] = dot_nn(back, jax.nn.gelu(mixed).astype(jnp.bfloat16)).astype(
            jnp.bfloat16
        )

    lax.fori_loop(near_middle, near_count, near_group, 0)
    for copy in weights[4:]:
        copy.wait()
    pieces = out_part.shape[0]
    piece_width = out_part.shape[2]

    def piece_cols(index):
        return pl.ds(pl.multiple_of(index * piece_width, piece_width), piece_width)

    most = 2 * width - LANES

    def state_piece(index, carry):
        state_part[:, piece_cols(index)] = dot_nn(
            act_ref[:, :most], w_out[:most, piece_cols(index)]
        )
        return carry

    def merge_pair(place_of, pair):
        cols = slice(pair * LANES, (pair + 1) * LANES)
        for goal in range(2, ranks):
            if OWNERS[pair] != goal:

                @pl.when(me == goal)
                def _():
                    far_copy(0, pair).wait_recv()

        @pl.when(me >= 2)
        def _():
            low = run_own[:, 2 * pair * LANES : (2 * pair + 1) * LANES]
            high = run_own[:, (2 * pair + 1) * LANES : (2 * pair + 2) * LANES]
            factor = jnp.exp2(-by_head(low, high, low.shape))
            acc_own[:, cols] += factor * far_land[:, cols].astype(jnp.float32)

        first = width + place_of * LANES
        act_ref[:, first : first + LANES] = head_rms(acc_own[:, cols]).astype(jnp.bfloat16)

    for place_of, pair in enumerate(MERGED[:-1]):
        merge_pair(place_of, pair)
    lax.fori_loop(0, pieces, state_piece, 0)
    merge_pair(pairs - 1, MERGED[-1])

    def part_copy(index):
        return pltpu.make_async_remote_copy(
            src_ref=out_part.at[index],
            dst_ref=out_arrived.at[index],
            send_sem=part_send.at[index],
            recv_sem=part_recv.at[index],
            **mate,
        )

    def piece_of(index, at):
        cols = piece_cols(index)
        return cols, state_part[at, cols] + dot_nn(act_ref[at, most:], w_out[most:, cols])

    def send_piece(index, carry):
        out_part[index] = piece_of(index, mate_rows)[1].astype(jnp.bfloat16)
        part_copy(index).start()
        return carry

    def own_piece(index, carry):
        cols, own = piece_of(index, own_rows)
        part_copy(index).wait_recv()
        out_ref[:, cols] = (own + out_arrived[index].astype(jnp.float32)).astype(jnp.bfloat16)
        return carry

    lax.fori_loop(0, pieces, send_piece, 0)
    lax.fori_loop(0, pieces, own_piece, 0)

    row_copy.wait_send()
    for index in range(pieces):
        part_copy(index).wait_send()
    for copy in end_copies:
        copy.wait_send()
    for origin in range(ranks):

        @pl.when(me == origin)
        def _(entries=sent[origin]):
            for entry in entries:
                (piece_copy if len(entry) > 1 else bias_copy)(*entry).wait_send()

    for pair in range(pairs):
        for slot in range(2):
            if OWNERS[pair] != slot + 2:

                @pl.when(me == OWNERS[pair])
                def _(pair=pair, slot=slot):
                    far_copy(slot, pair).wait_send()


def layer(ranks, tokens, norm_gain, weights, gains, key_bias, plan):
    count, features = tokens.shape
    width = weights[0].shape[1]
    rows = key_bias.shape[0]
    states = plan[0].size
    chunks = rows // LANES
    pairs = width // LANES
    pieces = features // 512
    bias = key_bias.T
    gains = [gain[None, :] for gain in gains]
    dma = pltpu.SemaphoreType.DMA
    vmem = pl.BlockSpec(memory_space=pltpu.VMEM)
    hbm = pl.BlockSpec(memory_space=pl.ANY)
    half, full = jnp.bfloat16, jnp.float32
    return pl.pallas_call(
        functools.partial(mixer_kernel, ranks),
        out_shape=jax.ShapeDtypeStruct((count, features), jnp.bfloat16),
        in_specs=[vmem] * 2 + [hbm] * 6 + [vmem] * (3 + len(plan)),
        out_specs=vmem,
        scratch_shapes=[
            pltpu.VMEM((4, *plan[0].shape), full),
            pltpu.VMEM((rows, features), half),
            pltpu.VMEM((2, states), full),
            pltpu.VMEM((rows, features), full),
            pltpu.VMEM((4, features, width), half),
            pltpu.VMEM((2 * width, features), half),
            pltpu.VMEM((rows, 2 * width), half),
            pltpu.VMEM((rows, width), half),
            pltpu.VMEM((rows, width), half),
            pltpu.VMEM((rows, width), half),
            pltpu.VMEM((rows, width), half),
            pltpu.VMEM((chunks, pairs, 2 * LANES), full),
            pltpu.VMEM((pieces, count, 512), half),
            pltpu.VMEM((pieces, count, 512), half),
            dma((5 + pairs,)),
            dma((2,)),
            dma((pieces,)),
            dma((pieces,)),
            pltpu.VMEM((2, rows, width), half),
            pltpu.VMEM((2, rows, width), half),
            pltpu.VMEM((2, rows, width), half),
            pltpu.VMEM((2, chunks, pairs, 2 * LANES), full),
            pltpu.VMEM((rows, states), full),
            pltpu.VMEM((rows, states), full),
            pltpu.VMEM((rows, width), half),
            pltpu.VMEM((8, states), full),
            pltpu.VMEM((8, states), full),
            pltpu.VMEM((ranks, 2, states), full),
            pltpu.VMEM((rows, width), full),
            pltpu.VMEM((rows, 2 * width), full),
            pltpu.VMEM((2 * rows, LANES), full),
            pltpu.VMEM((2 * rows, 2 * LANES), full),
            pltpu.VMEM((2, rows, width), half),
            pltpu.VMEM((rows, width), half),
            dma((3, 2, pairs, 2)),
            dma((3, 2, pairs, 2)),
            dma((len(BIASES),)),
            dma((2,)),
            dma((ranks,)),
            dma((ranks,)),
            dma((2, pairs)),
            dma((pairs,)),
        ],
        compiler_params=pltpu.CompilerParams(
            collective_id=0, has_side_effects=True, vmem_limit_bytes=58 * 2**20
        ),
        name="layer",
    )(tokens, norm_gain[None, :], *weights, *gains, bias, *plan)


def on_device(
    tokens,
    norm_gain,
    w_input,
    w_query,
    w_key,
    w_value,
    query_gain,
    key_gain,
    key_bias,
    eigen_real,
    eigen_imag,
    log_step,
    input_real,
    input_imag,
    read_real,
    read_imag,
    skip_gain,
    w_out_state,
    w_out_attn,
):
    ranks = lax.axis_size("sp")
    width = w_query.shape[1]
    rows = key_bias.shape[0]
    fits = (
        ranks == len(OWNERS)
        and width == ranks * LANES
        and w_input.shape[1] == width
        and width % 256 == 0
        and rows % LANES == 0
        and lax.axis_size("tp") == 2
        and tokens.shape[1] % 512 == 0
    )
    if not fits:
        return plain_device(
            tokens,
            norm_gain,
            w_input,
            w_query,
            w_key,
            w_value,
            query_gain,
            key_gain,
            key_bias,
            eigen_real,
            eigen_imag,
            log_step,
            input_real,
            input_imag,
            read_real,
            read_imag,
            skip_gain,
            w_out_state,
            w_out_attn,
        )
    plan = (
        eigen_real,
        eigen_imag,
        log_step[None, :],
        jnp.transpose(input_real, (0, 2, 1)).reshape(-1, STATE),
        jnp.transpose(input_imag, (0, 2, 1)).reshape(-1, STATE),
        read_real.reshape(-1, STATE),
        read_imag.reshape(-1, STATE),
        skip_gain[None, :],
    )
    weights = (w_input, w_query, w_key, w_value, w_out_state, w_out_attn)
    return layer(ranks, tokens, norm_gain, weights, (query_gain, key_gain), key_bias, plan)


def solution(mesh):
    placed = (
        P(("fs", "sp", "tp"), None),
        P(),
        P(None, "tp"),
        P(None, "tp"),
        P(None, "tp"),
        P(None, "tp"),
        P(),
        P(),
        P(("fs", "sp"), "tp"),
        P("tp", None),
        P("tp", None),
        P("tp"),
        P("tp", None, None),
        P("tp", None, None),
        P("tp", None, None),
        P("tp", None, None),
        P("tp"),
        P("tp", None),
        P("tp", None),
    )
    return jax.shard_map(
        on_device,
        mesh=mesh,
        in_specs=placed,
        out_specs=P(("fs", "sp", "tp"), None),
        check_vma=False,
    )
```
